512 devices in a mesh: sp: 64 (over z, y), tp: 8 (over x, core).
Axes of the slice: x: 4, y: 4, z: 16, core: 2. Of those that a mesh axis runs over, the one named last changes fastest.
Arguments:
- stream_in: bfloat16 [16384, 2048], P('sp'), may hold values from -6 to 6
- norm_gain: float32 [2, 2048], replicated, may hold values from 0.1 to 1.9
- value_weight: bfloat16 [2, 2048, 2048], P(None, 'sp', 'tp'), may hold values from -0.125 to 0.125
- gate_weight: bfloat16 [2, 2048, 2048], P(None, 'sp', 'tp'), may hold values from -0.125 to 0.125
- conv_taps: float32 [2, 31, 2048], P(None, None, 'tp'), may hold values from -5 to 5
- channel_gain: float32 [2, 2048], P(None, 'tp'), may hold values from 0.1 to 1.9
- out_weight: bfloat16 [2, 2048, 2048], P(None, 'tp', 'sp'), may hold values from -0.125 to 0.125
Outputs:
- stream_out: bfloat16 [16384, 2048], P('sp')
The draws below stay inside these ranges and needn't reach their ends.
All inputs are finite; a program needn't handle non-finite values.
Results may differ from the reference program's by a relative error of at most 0.015.
Values may be sent and summed in bfloat16 or wider, within the bound.
A program may use at most 64 MiB of HBM per device.

```python
import jax
import jax.numpy as jnp
from jax import lax

D = 2048
KERNEL = 31
LAYERS = 2
TOKENS = 16384


def draw_conv_taps(key, part):
    first, second = jax.random.split(jax.random.fold_in(key, 17))
    base = jnp.clip(jax.random.normal(first, (LAYERS, KERNEL, D), jnp.float32), -6.0, 6.0)
    blocks = jnp.exp(jax.random.uniform(second, (LAYERS, 1, 8), jnp.float32, -1.4, 1.4))
    scales = jnp.repeat(blocks, D // 8, axis=2)
    return base * scales / jnp.sqrt(jnp.float32(KERNEL))


def block_levels(key, shape, shards, low, top_value):
    def one(axis_at, parts):
        steps = jax.random.uniform(jax.random.fold_in(jax.random.fold_in(key, 6), axis_at), (parts,), jnp.float32, low / len(shards), top_value / len(shards))
        return jnp.repeat(jnp.exp(steps), shape[axis_at] // parts).reshape((-1,) + (1,) * (len(shape) - axis_at - 1))

    level = one(*shards[0])
    for cut in shards[1:]:
        level = level * one(*cut)
    return level


def scatter_about(rng, shape, width, limit, cuts=(), held_as=jnp.bfloat16):
    array = width * jax.random.normal(rng, shape, jnp.float32)
    if cuts:
        array = array * block_levels(rng, shape, cuts, -0.22, 0.18)
    return jnp.clip(array, -limit, limit).astype(held_as)


def setup_inputs(seed: int = 0) -> dict:
    splits = jax.random.split(jax.random.key(seed), 8)
    return {
        "stream_in": scatter_about(splits[0], (TOKENS, D), 1.0, 6.0, ((0, 64),)),
        "norm_gain": jnp.clip(1.0 + 0.18 * jax.random.normal(splits[1], (LAYERS, D), jnp.float32), 0.1, 1.9),
        "value_weight": scatter_about(splits[2], (LAYERS, D, D), D ** -0.5, 0.125, ((1, 64), (2, 8))),
        "gate_weight": scatter_about(splits[3], (LAYERS, D, D), D ** -0.5, 0.125, ((1, 64), (2, 8))),
        "conv_taps": draw_conv_taps(jax.random.fold_in(splits[7], 71), 0),
        "channel_gain": jnp.clip(1.0 + 0.18 * jax.random.normal(splits[5], (LAYERS, D), jnp.float32), 0.1, 1.9),
        "out_weight": scatter_about(splits[6], (LAYERS, D, D), D ** -0.5, 0.125, ((1, 8), (2, 64))),
    }


epsilon = 1e-05

def reference(stream_in, norm_gain, value_weight, gate_weight, conv_taps, channel_gain, out_weight):
    stream = stream_in
    for layer in range(LAYERS):
        wide = stream.astype(jnp.float32)
        normed = (wide * lax.rsqrt(lax.optimization_barrier(jnp.mean(wide * wide, axis=1, keepdims=True)) + epsilon) * norm_gain[layer]).astype(jnp.bfloat16)
        value = jnp.dot(normed, value_weight[layer], preferred_element_type=jnp.float32)
        gate = jnp.dot(normed, gate_weight[layer], preferred_element_type=jnp.float32)
        gated = (value * jax.nn.sigmoid(gate)).astype(jnp.bfloat16)
        padded = jnp.concatenate([jnp.zeros((KERNEL - 1, D), jnp.bfloat16), gated], axis=0).astype(jnp.float32)
        filtered = jnp.zeros((TOKENS, D), jnp.float32)
        for tap in range(KERNEL):
            filtered = filtered + conv_taps[layer, tap] * padded[tap:tap + TOKENS]
        mean_value = lax.optimization_barrier(jnp.mean(filtered, axis=1, keepdims=True))
        variance = lax.optimization_barrier(jnp.mean(filtered * filtered, axis=1, keepdims=True)) - mean_value * mean_value
        activated = jax.nn.silu((filtered - mean_value) * lax.rsqrt(variance + epsilon) * channel_gain[layer]).astype(jnp.bfloat16)
        branch = jnp.dot(activated, out_weight[layer], preferred_element_type=jnp.float32)
        stream = (wide + branch).astype(jnp.bfloat16)
    return stream
```

```python
import jax
import jax.numpy as jnp
from jax import lax
from jax.experimental import pallas as pl
from jax.experimental.pallas import tpu as pltpu
from jax.sharding import Mesh
from jax.sharding import PartitionSpec as P

Z, Y, X, C = 16, 4, 4, 2
TP = X * C
MESH = pl.DeviceIdType.MESH
EPS = 1e-05
F32 = jnp.float32
BF16 = jnp.bfloat16
N_SEMS = 560


def sigmoid(v):
    return 0.5 + 0.5 * jnp.tanh(0.5 * v)


def kernel(
    stream_hbm, ngain, vw, gw, taps, cgain, ow, out_ref,
    vg0, vg1, ou0, ou1, xs, s1, s2, f0, f1, nb, gx, h0, h1, gb0, gb1, cg, sems,
):
    z, y, x, c = (lax.axis_index(a) for a in ("z", "y", "x", "c"))
    tp = x * C + c
    sp = z * Y + y

    used = [0]
    sent = []

    def new_sem():
        used[0] += 1
        return sems.at[used[0] - 1]

    def remote(src, dst, device, keep=True):
        copy = pltpu.make_async_remote_copy(
            src_ref=src, dst_ref=dst, send_sem=new_sem(), recv_sem=new_sem(),
            device_id=device, device_id_type=MESH,
        )
        if keep:
            sent.append(copy)
        return copy

    def local(src, dst):
        copy = pltpu.make_async_copy(src, dst, new_sem())
        copy.start()
        return copy

    def zp(d):
        return lax.rem(z + d + Z, Z)

    def yp(d):
        return lax.rem(y + d + Y, Y)

    def xp(d):
        return lax.rem(x + d + X, X)

    own_vg0 = [local(vw.at[0], vg0.at[z, y, 0]), local(gw.at[0], vg0.at[z, y, 1])]
    own_vg1 = [local(vw.at[1], vg1.at[z, y, 0]), local(gw.at[1], vg1.at[z, y, 1])]
    own_xs = local(stream_hbm, xs)
    own_cg = local(cgain, cg.at[tp])

    zlo, zhi = lax.rem(z, TP), lax.div(z, TP)
    far = zlo != tp
    partner = (zhi * TP + tp, y, lax.div(zlo, C), lax.rem(zlo, C))
    nsp = lax.rem(sp + 1, Z * Y)
    psp = lax.rem(sp + Z * Y - 1, Z * Y)
    after = (lax.div(nsp, Y), lax.rem(nsp, Y), x, c)
    before = (lax.div(psp, Y), lax.rem(psp, Y), x, c)

    barrier = pltpu.get_barrier_semaphore()
    peers = [(zp(d), y, x, c) for d in (1, 2, -1, -2)] + [(z, yp(d), x, c) for d in (1, -1)]
    for d in range(1, TP):
        other = lax.rem(tp + d, TP)
        peers.append((z, y, lax.div(other, C), lax.rem(other, C)))
    peers += [after, before]
    for peer in peers:
        pl.semaphore_signal(barrier, inc=1, device_id=peer, device_id_type=MESH)

    @pl.when(far)
    def _():
        pl.semaphore_signal(barrier, inc=1, device_id=partner, device_id_type=MESH)

    pl.semaphore_wait(barrier, len(peers) + jnp.where(far, 1, 0))

    z_in = {}

    def z_send(m, buf, slot, direction, d):
        dist = 1 if d % 2 else 2
        at = buf.at[slot, y]
        copy = remote(at, at, (zp(direction * dist), y, x, c))
        copy.start()
        back = buf.at[zp(-direction * d), y]
        z_in[m, direction, d] = pltpu.make_async_remote_copy(
            src_ref=back, dst_ref=back, send_sem=copy.src_sem, recv_sem=copy.dst_sem,
            device_id=(z, y, x, c), device_id_type=MESH,
        )

    def z_stage(m, buf, s):
        for direction, most in ((1, Z // 2), (-1, Z // 2 - 1)):
            slot = zp(-direction * 2 * s)
            if s:
                z_in[m, direction, 2 * s].wait_recv()
            for d in (2 * s + 2, 2 * s + 1):
                if d <= most:
                    z_send(m, buf, slot, direction, d)

    y_in = {}
    y_far = {}

    def arriving(copy, at):
        return pltpu.make_async_remote_copy(
            src_ref=at, dst_ref=at, send_sem=copy.src_sem, recv_sem=copy.dst_sem,
            device_id=(z, y, x, c), device_id_type=MESH,
        )

    def y_send(m, buf, key, rows, plus, minus):
        for direction in (1, -1):
            at = buf.at[rows, y]
            copy = remote(at, at, (z, yp(direction), x, c))
            copy.start()
            y_in[m, key, direction] = arriving(copy, buf.at[rows, yp(-direction)])

    def y_relay(m, buf, key, piece):
        for direction in (1, -1):
            y_in[m, key, direction].wait_recv()
            at = piece(direction, yp(-direction))
            copy = remote(at, at, (z, yp(direction), x, c))
            copy.start()
            y_far[m, key, direction] = arriving(copy, piece(direction, yp(-2 * direction)))

    def y_done(m, key):
        for direction in (1, -1):
            y_far[m, key, direction].wait_recv()

    def half_of_pair(buf, rows):
        return lambda direction, row: buf.at[rows, row, 0 if direction == 1 else 1]

    def half_of_rows(buf):
        return lambda direction, row: buf.at[pl.ds(0 if direction == 1 else Z // 2, Z // 2), row]

    perm = []
    for layer, buf in ((0, ou0), (1, ou1)):
        there = buf.at[zhi * TP + tp, y, 0]
        perm.append(remote(ow.at[layer], there, partner, keep=False))
    perm_sem = [new_sem() for _ in range(2)]
    gains_in = []

    for copy in own_vg0:
        copy.wait()
    z_stage("vg0", vg0, 0)
    y_send("vg0", vg0, 0, z, None, None)

    @pl.when(far)
    def _():
        for copy in perm:
            copy.start()

    @pl.when(jnp.logical_not(far))
    def _():
        for layer, buf in ((0, ou0), (1, ou1)):
            pltpu.make_async_copy(ow.at[layer], buf.at[z, y, 0], perm_sem[layer]).start()

    for copy in own_vg1:
        copy.wait()
    z_stage("vg1", vg1, 0)

    own_cg.wait()
    for d in range(1, TP):
        to, frm = lax.rem(tp + d, TP), lax.rem(tp + TP - d, TP)
        copy = remote(cg.at[tp], cg.at[tp], (z, y, lax.div(to, C), lax.rem(to, C)))
        copy.start()
        gains_in.append(arriving(copy, cg.at[frm]))

    rows_all, width = xs.shape
    cols = gx.shape[2] * 2

    def group_of(layer, g, rows):
        if layer == 0:
            return xs[rows, pl.ds(g * 128, 128)]
        return s1[g % TP, g // TP, rows, :]

    def normalise(layer):
        step = 16

        @pl.loop(0, rows_all // step)
        def _(i):
            rows = pl.ds(pl.multiple_of(i * step, step), step)
            groups = [group_of(layer, g, rows).astype(F32) for g in range(width // 128)]
            total = groups[0] * groups[0]
            for g in groups[1:]:
                total = total + g * g
            scale = lax.rsqrt(jnp.sum(total, axis=1, keepdims=True) / width + EPS)
            for g, wide in enumerate(groups):
                gain = ngain[pl.ds(layer, 1), pl.ds(g * 128, 128)]
                nb[rows, pl.ds(g * 128, 128)] = (wide * scale * gain).astype(BF16)

    def project(layer, buf, gb):
        n = nb[...]
        value = jnp.dot(n, buf[:, :, 0].reshape(width, cols), preferred_element_type=F32)
        gate = jnp.dot(n, buf[:, :, 1].reshape(width, cols), preferred_element_type=F32)
        gated = (value * sigmoid(gate)).astype(BF16)
        gb[...] = gated[rows_all - 32 :]
        wide = gated.astype(F32)
        for h in range(2):
            gx[h, 32:, :] = wide[:, h * 128 : (h + 1) * 128]

    def convolve(layer, f, block):
        n = 64
        for h in range(2):
            acc = None
            for k in range(31):
                term = taps[layer, pl.ds(k, 1), pl.ds(h * 128, 128)] * gx[h, block * n + 2 + k : block * n + 2 + k + n, :]
                acc = term if acc is None else acc + term
            f[tp, block // 2, (block % 2) * n : (block % 2) * n + n, h * 128 : (h + 1) * 128] = acc.astype(BF16)

    def halo(layer, gb, hbuf):
        copy = remote(gb, hbuf, after, keep=False)

        @pl.when(sp < Z * Y - 1)
        def _():
            copy.start()

        return copy

    def halo_arrives(copy, hbuf):
        @pl.when(sp > 0)
        def _():
            copy.wait_recv()
            for h in range(2):
                gx[h, 0:32, :] = hbuf[:, h * 128 : (h + 1) * 128].astype(F32)

        @pl.when(sp == 0)
        def _():
            gx[:, 0:32, :] = jnp.zeros((2, 32, 128), F32)

    def halo_sent(copy):
        @pl.when(sp < Z * Y - 1)
        def _():
            copy.wait_send()

    def gather_tp(buf):
        me, other = buf.at[tp], (z, y, x, 1 - c)
        mate = tp + 1 - 2 * c

        def slot(d):
            return xp(d) * C + c

        def mate_slot(d):
            return xp(d) * C + 1 - c

        direct, passed = {}, []
        for direction in (1, -1):
            copy = remote(me, me, (z, y, xp(direction), c))
            copy.start()
            direct[direction] = arriving(copy, buf.at[slot(-direction)])
        copy = remote(me, me, other)
        copy.start()
        passed.append(arriving(copy, buf.at[mate]))
        relayed = {}
        for direction, half in ((1, 0), (-1, 1)):
            direct[direction].wait_recv()
            at = buf.at[slot(-direction), half]
            copy = remote(at, at, (z, y, xp(direction), c))
            copy.start()
            relayed[direction] = arriving(copy, buf.at[slot(2), half])
            at = buf.at[slot(-direction)]
            copy = remote(at, at, other)
            copy.start()
            passed.append(arriving(copy, buf.at[mate_slot(-direction)]))
        for direction, half in ((1, 0), (-1, 1)):
            relayed[direction].wait_recv()
            at = buf.at[slot(2), half]
            copy = remote(at, at, other)
            copy.start()
            passed.append(arriving(copy, buf.at[mate_slot(2), half]))
        for copy in passed:
            copy.wait_recv()

    def activate_and_project(layer, f, ou, nxt):
        n = rows_all // 2
        for half in range(2):
            first = second = jnp.zeros((n, 128), F32)
            for k in range(TP):
                for h in range(2):
                    part = f[k, half, :, h * 128 : (h + 1) * 128].astype(F32)
                    first = first + part
                    second = second + part * part
            mean = jnp.sum(first, axis=1, keepdims=True) / width
            var = jnp.sum(second, axis=1, keepdims=True) / width - mean * mean
            scale = lax.rsqrt(var + EPS)
            total = [jnp.zeros((n, 128), F32) for _ in range(2)]
            for k in range(TP):
                v = (f[k, half].astype(F32) - mean) * scale * cg[k, pl.ds(layer, 1), :]
                act = (v * sigmoid(v)).astype(BF16)
                for hi in range(2):
                    w = ou[hi * TP + k, :, 0].reshape(128, cols)
                    total[hi] = total[hi] + lax.dot_general(
                        act, w, (((1,), (1,)), ((), ())), preferred_element_type=F32
                    )
            for hi in range(2):
                rows = pl.ds(half * n, n)
                if layer == 0:
                    lane = pl.multiple_of((hi * TP + tp) * 128, 128)
                    old = xs[rows, pl.ds(lane, 128)]
                else:
                    old = s1[tp, hi, rows, :]
                nxt[tp, hi, rows, :] = (old.astype(F32) + total[hi]).astype(BF16)

    own_xs.wait()
    normalise(0)

    def new_keys(s):
        keys = []
        for direction, most in ((1, Z // 2), (-1, Z // 2 - 1)):
            keys += [direction * d for d in (2 * s, 2 * s - 1) if d <= most]
        return keys

    def pass_on(keys):
        for key in keys:
            d = abs(key)
            direction = 1 if key > 0 else -1
            if d % 2 or d == Z // 2:
                z_in["vg0", direction, d].wait_recv()
            y_send("vg0", vg0, key, zp(-key), None, None)

    def relay(keys):
        for key in keys:
            y_relay("vg0", vg0, key, half_of_pair(vg0, zp(-key)))

    old_keys = [0]
    for s in range(1, 4):
        z_stage("vg0", vg0, s)
        keys = new_keys(s)
        pass_on(keys)
        if s == 1:
            @pl.when(far)
            def _():
                for copy in perm:
                    copy.wait_recv()

            @pl.when(jnp.logical_not(far))
            def _():
                for layer, buf in ((0, ou0), (1, ou1)):
                    pltpu.make_async_copy(ow.at[layer], buf.at[z, y, 0], perm_sem[layer]).wait()

        relay(old_keys)
        old_keys = keys
        z_stage("ou0", ou0, s - 1)
        z_stage("vg1", vg1, s)
        z_stage("ou1", ou1, s - 1)
    keys = new_keys(4)
    pass_on(keys)
    relay(old_keys)
    z_stage("ou0", ou0, 3)
    z_stage("ou1", ou1, 3)
    relay(keys)
    every = [0] + [k for s in range(1, 5) for k in new_keys(s)]

    def z_rest(m, last_waited):
        for direction, most in ((1, Z // 2), (-1, Z // 2 - 1)):
            for d in range(1, most + 1):
                if d % 2 or d > last_waited:
                    z_in[m, direction, d].wait_recv()

    z_rest("ou0", 6)
    y_send("ou0", ou0, 0, pl.ds(0, Z), None, None)
    for key in every:
        y_done("vg0", key)

    project(0, vg0, gb0)
    copy0 = halo(0, gb0, h0)
    for b in (1, 2, 3):
        convolve(0, f0, b)
    halo_arrives(copy0, h0)
    convolve(0, f0, 0)
    y_relay("ou0", ou0, 0, half_of_rows(ou0))
    z_rest("vg1", 6)
    y_send("vg1", vg1, 0, pl.ds(0, Z), None, None)
    gather_tp(f0)
    for copy in gains_in:
        copy.wait_recv()
    y_done("ou0", 0)
    activate_and_project(0, f0, ou0, s1)
    gather_tp(s1)
    normalise(1)
    y_relay("vg1", vg1, 0, half_of_pair(vg1, pl.ds(0, Z)))
    z_rest("ou1", 6)
    y_send("ou1", ou1, 0, pl.ds(0, Z), None, None)
    y_done("vg1", 0)

    project(1, vg1, gb1)
    copy1 = halo(1, gb1, h1)
    for b in (1, 2, 3):
        convolve(1, f1, b)
    halo_arrives(copy1, h1)
    convolve(1, f1, 0)
    gather_tp(f1)
    y_relay("ou1", ou1, 0, half_of_rows(ou1))
    y_done("ou1", 0)
    activate_and_project(1, f1, ou1, s2)
    gather_tp(s2)
    for g in range(width // 128):
        out_ref[:, g * 128 : (g + 1) * 128] = s2[g % TP, g // TP]

    for copy in sent:
        copy.wait_send()
    halo_sent(copy0)
    halo_sent(copy1)

    @pl.when(far)
    def _():
        for copy in perm:
            copy.wait_send()

    assert used[0] <= N_SEMS, used[0]


def body(stream_in, norm_gain, value_weight, gate_weight, conv_taps, channel_gain, out_weight):
    rows, width = stream_in.shape
    depth, cols = value_weight.shape[1:]
    any_, vmem = pl.BlockSpec(memory_space=pl.ANY), pl.BlockSpec(memory_space=pltpu.VMEM)
    out_t = jnp.swapaxes(out_weight, 1, 2)
    return pl.pallas_call(
        kernel,
        out_shape=jax.ShapeDtypeStruct((rows, width), BF16),
        in_specs=[any_, vmem, any_, any_, vmem, any_, any_],
        out_specs=vmem,
        scratch_shapes=[
            pltpu.VMEM((Z, Y, 2, depth, cols), BF16),
            pltpu.VMEM((Z, Y, 2, depth, cols), BF16),
            pltpu.VMEM((Z, Y, 1, depth, cols), BF16),
            pltpu.VMEM((Z, Y, 1, depth, cols), BF16),
            pltpu.VMEM((rows, width), BF16),
            pltpu.VMEM((TP, 2, rows, 128), BF16),
            pltpu.VMEM((TP, 2, rows, 128), BF16),
            pltpu.VMEM((TP, 2, rows // 2, cols), BF16),
            pltpu.VMEM((TP, 2, rows // 2, cols), BF16),
            pltpu.VMEM((rows, width), BF16),
            pltpu.VMEM((2, rows + 32, 128), F32),
            pltpu.VMEM((32, cols), BF16),
            pltpu.VMEM((32, cols), BF16),
            pltpu.VMEM((32, cols), BF16),
            pltpu.VMEM((32, cols), BF16),
            pltpu.VMEM((TP, 2, cols), F32),
            pltpu.SemaphoreType.DMA((N_SEMS,)),
        ],
        compiler_params=pltpu.CompilerParams(
            collective_id=0, has_side_effects=True, vmem_limit_bytes=48 * 1024 * 1024
        ),
    )(stream_in, norm_gain, value_weight, gate_weight, conv_taps, channel_gain, out_t)


def solution(mesh):
    finer = Mesh(mesh.devices.reshape(Z, Y, X, C), ("z", "y", "x", "c"))
    sp, tp = ("z", "y"), ("x", "c")
    placed = (
        P(sp, None),
        P(),
        P(None, sp, tp),
        P(None, sp, tp),
        P(None, None, tp),
        P(None, tp),
        P(None, tp, sp),
    )
    return jax.shard_map(body, mesh=finer, in_specs=placed, out_specs=P(sp, None), check_vma=False)
```

```python
import jax
import jax.numpy as jnp
from jax import lax
from jax.experimental import pallas as pl
from jax.experimental.pallas import tpu as pltpu
from jax.sharding import Mesh
from jax.sharding import PartitionSpec as P

Z, Y, X, C = 16, 4, 4, 2
TP = X * C
MESH = pl.DeviceIdType.MESH
EPS = 1e-05
F32 = jnp.float32
BF16 = jnp.bfloat16
N_SEMS = 106
HALO = 32
RING = [
    [(2 * s, tuple(d for d in (2 * s + 2, 2 * s + 1) if d <= Z // 2)),
     (-2 * s, tuple(-d for d in (2 * s + 2, 2 * s + 1) if d < Z // 2))]
    for s in range(4)
]
VMEM_LIMIT = 67043328
scope = jax.named_scope


def sigmoid(v):
    return 0.5 + 0.5 * jnp.tanh(0.5 * v)


def kernel(
    stream_hbm, ngain, vw, gw, taps, cgain, ow, out_ref,
    vg0, vg1, ou0, ou1, xs, s1, s2, f0, f1, nb, gx, h0, h1, gb0, gb1, cg, sems,
):
    z, y, x, c = (lax.axis_index(a) for a in ("z", "y", "x", "c"))
    tp = x * C + c
    sp = z * Y + y
    used = [0]

    def new_sem():
        used[0] += 1
        return sems.at[used[0] - 1]

    def send(src, dst, device, send_sem, recv_sem):
        pltpu.make_async_remote_copy(
            src_ref=src, dst_ref=dst, send_sem=send_sem, recv_sem=recv_sem,
            device_id=device, device_id_type=MESH,
        ).start()

    def wait(ref, sem):
        pltpu.make_async_copy(ref, ref, sem).wait()

    drains = []

    def send_group(ref):
        sem = new_sem()
        drains.append((ref, sem))
        return sem

    def zp(d):
        return lax.rem(z + d + Z, Z)

    def yp(d):
        return lax.rem(y + d + Y, Y)

    def xp(d):
        return lax.rem(x + d + X, X)

    own_sem = [new_sem() for _ in range(4)]
    own = [
        pltpu.make_async_copy(vw.at[0], vg0.at[z, y, 0], own_sem[0]),
        pltpu.make_async_copy(gw.at[0], vg0.at[z, y, 1], own_sem[0]),
        pltpu.make_async_copy(vw.at[1], vg1.at[z, y, 0], own_sem[1]),
        pltpu.make_async_copy(gw.at[1], vg1.at[z, y, 1], own_sem[1]),
        pltpu.make_async_copy(stream_hbm, xs, own_sem[2]),
        pltpu.make_async_copy(cgain, cg.at[tp], own_sem[3]),
    ]
    for copy in own:
        copy.start()

    zlo, zhi = lax.rem(z, TP), lax.div(z, TP)
    far = zlo != tp
    partner = (zhi * TP + tp, y, lax.div(zlo, C), lax.rem(zlo, C))
    nsp = lax.rem(sp + 1, Z * Y)
    psp = lax.rem(sp + Z * Y - 1, Z * Y)
    after = (lax.div(nsp, Y), lax.rem(nsp, Y), x, c)
    before = (lax.div(psp, Y), lax.rem(psp, Y), x, c)

    barrier = pltpu.get_barrier_semaphore()
    peers = [(zp(d), y, x, c) for d in (1, 2, -1, -2)] + [(z, yp(d), x, c) for d in (1, -1, 2)]
    for d in range(1, TP):
        other = lax.rem(tp + d, TP)
        peers.append((z, y, lax.div(other, C), lax.rem(other, C)))
    peers += [after, before]
    for peer in peers:
        pl.semaphore_signal(barrier, inc=1, device_id=peer, device_id_type=MESH)

    @pl.when(far)
    def _():
        pl.semaphore_signal(barrier, inc=1, device_id=partner, device_id_type=MESH)

    with scope("barrier"):
        pl.semaphore_wait(barrier, len(peers) + jnp.where(far, 1, 0))

    z_sems = {}

    def brought(plan, s):
        return [d for _, news in plan[s] for d in news]

    def z_block(buf, slot, part):
        return buf.at[slot, y] if part is None else buf.at[slot, y, part]

    def z_stage(m, buf, plan, s, part=None):
        if s == 0:
            z_sems[m, part] = [new_sem() for _ in plan], send_group(z_blocks(buf, Z - 1, part))
        sems_in, out = z_sems[m, part]
        for d, news in plan[s]:
            at = z_block(buf, zp(-d), part)
            for new in news:
                send(at, at, (zp(new - d), y, x, c), out, sems_in[s])

    def z_blocks(buf, n, part):
        return buf.at[pl.ds(0, n), 0] if part is None else buf.at[pl.ds(0, n), 0, part]

    def z_wait(m, buf, plan, s, part=None):
        wait(z_blocks(buf, len(brought(plan, s)), part), z_sems[m, part][0][s])

    y_sems = {}

    def y_group(m, buf):
        pair = buf.shape[2] == 2
        sent, passed = send_group(buf.at[:, pl.ds(0, 2)]), send_group(buf.at[:, 0])
        y_sems[m] = sent, passed, new_sem(), {}

        def half(slot, row, h):
            return buf.at[slot, row, h] if pair else buf.at[slot, row, 0, pl.ds(h * 16, 16)]

        def pass_on(key, ds):
            first, second = new_sem(), new_sem()
            y_sems[m][3][key] = first, second
            for d in ds:
                at = buf.at[zp(-d), y]
                send(at, at, (z, yp(1), x, c), sent, first)
                send(at, at, (z, yp(-1), x, c), sent, second)

        def relay(key, ds):
            for direction, h, sem in ((1, 0, y_sems[m][3][key][0]), (-1, 1, y_sems[m][3][key][1])):
                wait(buf.at[pl.ds(0, len(ds)), 0], sem)
                for d in ds:
                    at = half(zp(-d), yp(-direction), h)
                    send(at, at, (z, yp(direction), x, c), passed, y_sems[m][2])

        def pass_far(key, ds):
            pass_on(key, ds)
            for d in ds:
                at = buf.at[zp(-d), y]
                send(at, at, (z, yp(2), x, c), passed, y_sems[m][2])

        def near_done(key, ds):
            for sem in y_sems[m][3][key]:
                wait(buf.at[pl.ds(0, len(ds)), 0], sem)

        def done():
            wait(buf.at[:, 0], y_sems[m][2])

        return pass_on, relay, pass_far, near_done, done

    mine = lax.rem(z, 2)

    def spread(m, buf):
        pair = buf.shape[2] == 2
        quarter = pl.ds(0, Z // 2)
        whole = buf.at[:, 0, 0] if pair else buf.at[quarter, 0, 0]
        part_half = buf.at[quarter, 0, 0] if pair else buf.at[pl.ds(0, Z // 4), 0, 0]
        all3 = buf.at[:, pl.ds(0, 3), 0] if pair else buf.at[quarter, pl.ds(0, 3), 0]
        sent = send_group(buf.at[:, 0] if pair else buf.at[:, 0, 0])
        passed = send_group(whole)
        swapped = send_group(all3)
        row_in, far_in, swap_in = [new_sem(), new_sem()], [new_sem(), new_sem()], new_sem()
        ways = ((1, 0), (-1, 1))

        def piece(row, part, half=None):
            if pair:
                n = Z if half is None else Z // 2
                return buf.at[pl.ds((half or 0) * Z // 2, n), row, part]
            n = Z // 2 if half is None else Z // 4
            return buf.at[pl.ds(part * (Z // 2) + (half or 0) * Z // 4, n), row, 0]

        def a():
            for direction, h in ways:
                send(piece(y, mine), piece(y, mine), (z, yp(direction), x, c), sent, row_in[h])

        def b():
            for direction, h in ways:
                wait(whole, row_in[h])
                at = piece(yp(-direction), mine, h)
                send(at, at, (z, yp(direction), x, c), passed, far_in[h])
            for direction, h in ways:
                at = piece(yp(-direction), mine)
                send(at, at, (zp(direction), y, x, c), swapped, swap_in)

        def e():
            for direction, h in ways:
                wait(part_half, far_in[h])
                at = piece(yp(2), mine, h)
                send(at, at, (zp(direction), y, x, c), swapped, swap_in)

        def done():
            wait(all3, swap_in)

        return a, b, e, done

    def gather_tp(buf, h):
        me, other = buf.at[tp, h], (z, y, x, 1 - c)
        out = send_group(buf.at[pl.ds(0, TP - 1), h])
        near_in, far_in, mate = new_sem(), new_sem(), new_sem()

        def slot(d):
            return buf.at[xp(d) * C + c, h]

        def begin():
            for d, sem in ((2, far_in), (1, near_in), (-1, near_in)):
                send(me, me, (z, y, xp(d), c), out, sem)
            send(me, me, other, out, mate)

        def near():
            wait(buf.at[pl.ds(0, 2), h], near_in)
            for d in (1, -1):
                send(slot(d), slot(d), other, out, mate)

        def last():
            wait(me, far_in)
            send(slot(2), slot(2), other, out, mate)

        def done():
            wait(buf.at[pl.ds(0, X), h], mate)

        return begin, near, last, done

    rows_all, width = xs.shape
    cols = gx.shape[2] * 2
    nh = rows_all // 2

    def normalise(layer, h):
        n = 64
        for i in range(nh // n):
            rows = pl.ds(h * nh + i * n, n)

            def group(g):
                if layer == 0:
                    return xs[rows, pl.ds(g * 128, 128)].astype(F32)
                return s1[g % TP, h, g // TP, pl.ds(i * n, n), :].astype(F32)

            total = None
            for g in range(width // 128):
                wide = group(g)
                total = wide * wide if total is None else total + wide * wide
            scale = lax.rsqrt(jnp.sum(total, axis=1, keepdims=True) / width + EPS)
            for g in range(width // 128):
                gain = ngain[pl.ds(layer, 1), pl.ds(g * 128, 128)]
                nb[rows, pl.ds(g * 128, 128)] = (group(g) * scale * gain).astype(BF16)

    def project(layer, buf, gb, h):
        n = nb[pl.ds(h * nh, nh), :]
        value = jnp.dot(n, buf[:, :, 0].reshape(width, cols), preferred_element_type=F32)
        gate = jnp.dot(n, buf[:, :, 1].reshape(width, cols), preferred_element_type=F32)
        gated = (value * sigmoid(gate)).astype(BF16)
        if h:
            gb[...] = gated[nh - HALO :]
        wide = gated.astype(F32)
        for j in range(2):
            gx[j, HALO + h * nh : HALO + h * nh + nh, :] = wide[:, j * 128 : (j + 1) * 128]

    def convolve(layer, f, block):
        n = 64
        first = block * n + HALO - 30
        for j in range(2):
            acc = None
            for k in range(31):
                term = taps[k, pl.ds(layer, 1), pl.ds(j * 128, 128)] * gx[j, first + k : first + k + n, :]
                acc = term if acc is None else acc + term
            f[tp, block // 2, (block % 2) * n : (block % 2) * n + n, j * 128 : (j + 1) * 128] = acc.astype(BF16)

    def halo(gb, hbuf):
        copy = pltpu.make_async_remote_copy(
            src_ref=gb, dst_ref=hbuf, send_sem=new_sem(), recv_sem=new_sem(),
            device_id=after, device_id_type=MESH,
        )

        @pl.when(sp < Z * Y - 1)
        def _():
            copy.start()

        def arrives():
            @pl.when(sp > 0)
            def _():
                copy.wait_recv()
                for j in range(2):
                    gx[j, 0:HALO, :] = hbuf[:, j * 128 : (j + 1) * 128].astype(F32)

            @pl.when(sp == 0)
            def _():
                gx[:, 0:HALO, :] = jnp.zeros((2, HALO, 128), F32)

        def sent():
            @pl.when(sp < Z * Y - 1)
            def _():
                copy.wait_send()

        return arrives, sent

    def activate_and_project(layer, f, ou, nxt, h):
        first = second = jnp.zeros((nh, 128), F32)
        for k in range(TP):
            for j in range(2):
                part = f[k, h, :, j * 128 : (j + 1) * 128].astype(F32)
                first = first + part
                second = second + part * part
        mean = jnp.sum(first, axis=1, keepdims=True) / width
        var = jnp.sum(second, axis=1, keepdims=True) / width - mean * mean
        scale = lax.rsqrt(var + EPS)
        total = [jnp.zeros((nh, 128), F32) for _ in range(2)]
        for k in range(TP):
            v = (f[k, h].astype(F32) - mean) * scale * cg[k, pl.ds(layer, 1), :]
            act = (v * sigmoid(v)).astype(BF16)
            for hi in range(2):
                w = ou[hi * TP + k, :, 0].reshape(128, cols)
                total[hi] = total[hi] + lax.dot_general(
                    act, w, (((1,), (1,)), ((), ())), preferred_element_type=F32
                )
        for hi in range(2):
            if layer == 0:
                lane = pl.multiple_of((hi * TP + tp) * 128, 128)
                old = xs[pl.ds(h * nh, nh), pl.ds(lane, 128)]
            else:
                old = s1[tp, h, hi]
            nxt[tp, h, hi] = (old.astype(F32) + total[hi]).astype(BF16)

    perm_send = send_group(ow)
    perm_recv = new_sem()
    perm = [
        pltpu.make_async_remote_copy(
            src_ref=ow.at[layer], dst_ref=buf.at[zhi * TP + tp, y, 0], send_sem=perm_send, recv_sem=perm_recv,
            device_id=partner, device_id_type=MESH,
        )
        for layer, buf in ((0, ou0), (1, ou1))
    ]
    drains.pop()
    stay = [pltpu.make_async_copy(ow.at[layer], buf.at[z, y, 0], perm_recv) for layer, buf in ((0, ou0), (1, ou1))]

    def perm_start():
        @pl.when(far)
        def _():
            for copy in perm:
                copy.start()

        @pl.when(jnp.logical_not(far))
        def _():
            for copy in stay:
                copy.start()

    def perm_done():
        wait(ow, perm_recv)

    pass_vg, relay_vg, far_vg, near_vg, done_vg = y_group("vg0", vg0)
    ou0_a, ou0_b, ou0_c, ou0_done = spread("ou0", ou0)
    vg1_a, vg1_b, vg1_c, vg1_done = spread("vg1", vg1)
    ou1_a, ou1_b, ou1_c, ou1_done = spread("ou1", ou1)

    def vg0_stage(s):
        for part in range(2):
            if s:
                z_wait("vg0", vg0, RING, s - 1, part)
            if s < 4:
                z_stage("vg0", vg0, RING, s, part)

    wait(vg0.at[z, y], own_sem[0])
    vg0_stage(0)
    pass_vg(0, [0])
    perm_start()
    wait(vg1.at[z, y], own_sem[1])
    z_stage("vg1", vg1, RING, 0)
    wait(cg.at[tp], own_sem[3])
    gain_sent, gain_in = send_group(cg.at[pl.ds(0, TP - 1)]), new_sem()
    for d in range(1, TP):
        to = lax.rem(tp + d, TP)
        send(cg.at[tp], cg.at[tp], (z, y, lax.div(to, C), lax.rem(to, C)), gain_sent, gain_in)
    wait(xs, own_sem[2])
    with scope("norm0"):
        for h in range(2):
            normalise(0, h)

    ring = [[0]] + [brought(RING, s) for s in range(4)]

    def ring_step(m, buf, s):
        z_wait(m, buf, RING, s - 1)
        if s < 4:
            z_stage(m, buf, RING, s)

    with scope("stage1"):
        vg0_stage(1)
        pass_vg(1, ring[1])
        relay_vg(0, ring[0])
    with scope("stage2"):
        vg0_stage(2)
        pass_vg(2, ring[2])
        relay_vg(1, ring[1])
        perm_done()
        z_stage("ou0", ou0, RING, 0)
        ring_step("vg1", vg1, 1)
    with scope("stage3"):
        vg0_stage(3)
        pass_vg(3, ring[3])
        relay_vg(2, ring[2])
        ring_step("ou0", ou0, 1)
        ring_step("vg1", vg1, 2)
    with scope("stage4"):
        vg0_stage(4)
        far_vg(4, ring[4])
        relay_vg(3, ring[3])
        ring_step("ou0", ou0, 2)
        ring_step("vg1", vg1, 3)
        z_stage("ou1", ou1, RING, 0)
    with scope("stage5"):
        ring_step("ou0", ou0, 3)
    with scope("vg0done"):
        near_vg(4, ring[4])
        done_vg()

    def layer_head(layer, vg, gb, hbuf, f, ready):
        first, second = gather_tp(f, 1), gather_tp(f, 0)
        with scope("proj"):
            project(layer, vg, gb, 1)
        arrives, sent = halo(gb, hbuf)
        with scope("projb"):
            ready()
            project(layer, vg, gb, 0)
        with scope("conv"):
            convolve(layer, f, 2)
            convolve(layer, f, 3)
        first[0]()
        with scope("convb"):
            convolve(layer, f, 1)
        return first, second, arrives, sent

    def layer_tail(layer, f, ou, nxt, parts, arrives, hooks):
        first, second = parts
        with scope("hook0"):
            hooks[0]()
        with scope("halo"):
            arrives()
            convolve(layer, f, 0)
        second[0]()
        with scope("hook0b"):
            hooks[1]()
        with scope("ag1"):
            first[1]()
            second[1]()
        with scope("hook1"):
            hooks[2]()
        with scope("ag1b"):
            first[2]()
            first[3]()
        with scope("hook2"):
            hooks[3]()
        first2, second2 = gather_tp(nxt, 1), gather_tp(nxt, 0)
        with scope("act"):
            activate_and_project(layer, f, ou, nxt, 1)
        first2[0]()
        with scope("ag1c"):
            second[2]()
            second[3]()
        with scope("actb"):
            activate_and_project(layer, f, ou, nxt, 0)
        second2[0]()
        with scope("hook3"):
            hooks[4]()
        with scope("ag2"):
            first2[1]()
            second2[1]()
        with scope("hook4"):
            hooks[5]()
        with scope("ag2b"):
            first2[2]()
            first2[3]()
        return second2

    def nothing():
        pass

    first, second, arrives, sent0 = layer_head(0, vg0, gb0, h0, f0, nothing)

    def hook00():
        ring_step("ou0", ou0, 4)
        ou0_a()
        ring_step("vg1", vg1, 4)
        vg1_a()
        ring_step("ou1", ou1, 1)

    def hook00b():
        ring_step("ou1", ou1, 2)
        ou0_b()

    def hook01():
        ou0_c()
        ring_step("ou1", ou1, 3)

    def hook02():
        vg1_b()
        wait(cg.at[pl.ds(0, TP - 1)], gain_in)
        ou0_done()

    def hook03():
        ring_step("ou1", ou1, 4)
        vg1_c()
        ou1_a()

    rest = layer_tail(0, f0, ou0, s1, (first, second), arrives, (hook00, hook00b, hook01, hook02, hook03, nothing))
    with scope("norm1"):
        normalise(1, 1)

    def ready():
        with scope("ag2c"):
            rest[2]()
            rest[3]()
        normalise(1, 0)

    with scope("vg1done"):
        vg1_done()

    first, second, arrives, sent1 = layer_head(1, vg1, gb1, h1, f1, ready)
    rest1 = layer_tail(
        1, f1, ou1, s2, (first, second), arrives, (nothing, ou1_b, ou1_c, ou1_done, nothing, nothing)
    )

    def write(h):
        for g in range(width // 128):
            out_ref[h * nh : (h + 1) * nh, g * 128 : (g + 1) * 128] = s2[g % TP, h, g // TP]

    write(1)
    with scope("ag2c"):
        rest1[2]()
        rest1[3]()
    write(0)

    with scope("out"):
        for ref, sem in drains:
            wait(ref, sem)
        sent0()
        sent1()

        @pl.when(far)
        def _():
            wait(ow, perm_send)

    assert used[0] == N_SEMS, used[0]


def body(stream_in, norm_gain, value_weight, gate_weight, conv_taps, channel_gain, out_weight):
    rows, width = stream_in.shape
    depth, cols = value_weight.shape[1:]
    hbm, vmem = pl.BlockSpec(memory_space=pltpu.HBM), pl.BlockSpec(memory_space=pltpu.VMEM)
    out_t = jnp.swapaxes(out_weight, 1, 2)
    taps = jnp.swapaxes(conv_taps, 0, 1)
    return pl.pallas_call(
        kernel,
        out_shape=jax.ShapeDtypeStruct((rows, width), BF16),
        in_specs=[hbm, vmem, hbm, hbm, vmem, hbm, hbm],
        out_specs=vmem,
        scratch_shapes=[
            pltpu.VMEM((Z, Y, 2, depth, cols), BF16),
            pltpu.VMEM((Z, Y, 2, depth, cols), BF16),
            pltpu.VMEM((Z, Y, 1, depth, cols), BF16),
            pltpu.VMEM((Z, Y, 1, depth, cols), BF16),
            pltpu.VMEM((rows, width), BF16),
            pltpu.VMEM((TP, 2, 2, rows // 2, 128), BF16),
            pltpu.VMEM((TP, 2, 2, rows // 2, 128), BF16),
            pltpu.VMEM((TP, 2, rows // 2, cols), BF16),
            pltpu.VMEM((TP, 2, rows // 2, cols), BF16),
            pltpu.VMEM((rows, width), BF16),
            pltpu.VMEM((2, rows + HALO, 128), F32),
            pltpu.VMEM((HALO, cols), BF16),
            pltpu.VMEM((HALO, cols), BF16),
            pltpu.VMEM((HALO, cols), BF16),
            pltpu.VMEM((HALO, cols), BF16),
            pltpu.VMEM((TP, 2, cols), F32),
            pltpu.SemaphoreType.DMA((N_SEMS,)),
        ],
        compiler_params=pltpu.CompilerParams(
            collective_id=0, has_side_effects=True, vmem_limit_bytes=VMEM_LIMIT
        ),
    )(stream_in, norm_gain, value_weight, gate_weight, taps, channel_gain, out_t)


def solution(mesh):
    finer = Mesh(mesh.devices.reshape(Z, Y, X, C), ("z", "y", "x", "c"))
    sp, tp = ("z", "y"), ("x", "c")
    placed = (
        P(sp, None),
        P(),
        P(None, sp, tp),
        P(None, sp, tp),
        P(None, None, tp),
        P(None, tp),
        P(None, tp, sp),
    )
    return jax.shard_map(body, mesh=finer, in_specs=placed, out_specs=P(sp, None), check_vma=False)
```

```python
import jax
import jax.numpy as jnp
from jax import lax
from jax.experimental import pallas as pl
from jax.experimental.pallas import tpu as pltpu
from jax.sharding import Mesh
from jax.sharding import PartitionSpec as P

Z, Y, X, C = 16, 4, 4, 2
TP = X * C
MESH = pl.DeviceIdType.MESH
EPS = 1e-05
F32 = jnp.float32
BF16 = jnp.bfloat16
N_SEMS = 113
HALO = 32
RING = [
    [(2 * s, tuple(d for d in (2 * s + 2, 2 * s + 1) if d <= Z // 2)),
     (-2 * s, tuple(-d for d in (2 * s + 2, 2 * s + 1) if d < Z // 2))]
    for s in range(4)
]
VMEM_LIMIT = 60_000_000
scope = jax.named_scope


def sigmoid(v):
    return 0.5 + 0.5 * jnp.tanh(0.5 * v)


def kernel(
    stream_hbm, ngain, vw, gw, taps, cgain, ow, out_ref,
    vg0, vg1, ou0, ou1, xs, s1, s2, f0, f1, nb, gx, h0, h1, gb0, gb1, cg, sems,
):
    z, y, x, c = (lax.axis_index(a) for a in ("z", "y", "x", "c"))
    tp = x * C + c
    sp = z * Y + y
    used = [0]

    def new_sem():
        used[0] += 1
        return sems.at[used[0] - 1]

    def send(src, dst, device, send_sem, recv_sem):
        pltpu.make_async_remote_copy(
            src_ref=src, dst_ref=dst, send_sem=send_sem, recv_sem=recv_sem,
            device_id=device, device_id_type=MESH,
        ).start()

    def wait(ref, sem):
        pltpu.make_async_copy(ref, ref, sem).wait()

    drains = []

    def send_group(ref):
        sem = new_sem()
        drains.append((ref, sem))
        return sem

    def zp(d):
        return lax.rem(z + d + Z, Z)

    def yp(d):
        return lax.rem(y + d + Y, Y)

    def xp(d):
        return lax.rem(x + d + X, X)

    own_sem = [new_sem() for _ in range(4)]
    own = [
        pltpu.make_async_copy(vw.at[0], vg0.at[z, y, 0], own_sem[0]),
        pltpu.make_async_copy(gw.at[0], vg0.at[z, y, 1], own_sem[0]),
        pltpu.make_async_copy(vw.at[1], vg1.at[z, y, 0], own_sem[1]),
        pltpu.make_async_copy(gw.at[1], vg1.at[z, y, 1], own_sem[1]),
        pltpu.make_async_copy(stream_hbm, xs, own_sem[2]),
        pltpu.make_async_copy(cgain, cg.at[tp], own_sem[3]),
    ]
    for copy in own:
        copy.start()

    zlo = lax.rem(z, TP)
    far = zlo != tp
    to_z = zp(lax.rem(tp - zlo + 12, TP) - 4)
    from_z = zp(4 - lax.rem(zlo - tp + 12, TP))
    goes_to = (to_z, y, lax.div(zlo, C), lax.rem(zlo, C))
    comes_from = (from_z, y, lax.div(zlo, C), lax.rem(zlo, C))
    nsp = lax.rem(sp + 1, Z * Y)
    psp = lax.rem(sp + Z * Y - 1, Z * Y)
    after = (lax.div(nsp, Y), lax.rem(nsp, Y), x, c)
    before = (lax.div(psp, Y), lax.rem(psp, Y), x, c)

    barrier = pltpu.get_barrier_semaphore()
    peers = [(zp(d), y, x, c) for d in (1, 2, -1, -2)] + [(z, yp(d), x, c) for d in (1, -1, 2)]
    for d in range(1, TP):
        other = lax.rem(tp + d, TP)
        peers.append((z, y, lax.div(other, C), lax.rem(other, C)))
    peers += [after, before]
    for peer in peers:
        pl.semaphore_signal(barrier, inc=1, device_id=peer, device_id_type=MESH)

    @pl.when(far)
    def _():
        pl.semaphore_signal(barrier, inc=1, device_id=comes_from, device_id_type=MESH)

    with scope("barrier"):
        pl.semaphore_wait(barrier, len(peers) + jnp.where(far, 1, 0))

    def block(buf, slot, row, part=None):
        if buf.shape[0] != Z:
            return buf.at[lax.div(slot, 2), lax.rem(slot, 2), row]
        return buf.at[slot, row] if part is None else buf.at[slot, row, part]

    def blocks(buf, n, part=None):
        if buf.shape[0] != Z:
            return buf.at[pl.ds(0, max(1, n // 3)), 0, pl.ds(0, 3)] if n % 3 == 0 else buf.at[pl.ds(0, 1), 0, pl.ds(0, n)]
        return buf.at[pl.ds(0, n), 0] if part is None else buf.at[pl.ds(0, n), 0, part]

    z_sems = {}

    def brought(plan, s):
        return [d for _, news in plan[s] for d in news]

    def z_stage(m, buf, plan, s, part=None):
        if s == 0:
            z_sems[m, part] = [new_sem() for _ in plan], send_group(blocks(buf, Z - 1, part))
        sems_in, out = z_sems[m, part]
        for d, news in plan[s]:
            at = block(buf, zp(-d), y, part)
            for new in news:
                send(at, at, (zp(new - d), y, x, c), out, sems_in[s])

    def z_wait(m, buf, plan, s, part=None):
        wait(blocks(buf, len(brought(plan, s)), part), z_sems[m, part][0][s])

    def y_group(m, buf):
        pair = buf.shape[0] == Z
        sent = send_group(buf.at[:, pl.ds(0, 2)] if pair else buf.at[pl.ds(0, 4), 0])
        far_bytes = buf.at[:, 0] if pair else buf.at[pl.ds(0, 2), 0]
        passed, far_in, near_in = send_group(far_bytes), new_sem(), {}

        def half(slot, row, h):
            return buf.at[slot, row, h] if pair else block(buf, slot, row).at[pl.ds(h * 16, 16)]

        def pass_on(key, ds):
            near_in[key] = new_sem(), new_sem()
            for d in ds:
                at = block(buf, zp(-d), y)
                for direction, sem in zip((1, -1), near_in[key]):
                    send(at, at, (z, yp(direction), x, c), sent, sem)

        def relay(key, ds):
            for direction, h in ((1, 0), (-1, 1)):
                wait(blocks(buf, len(ds)), near_in[key][h])
                for d in ds:
                    at = half(zp(-d), yp(-direction), h)
                    send(at, at, (z, yp(direction), x, c), passed, far_in)

        def pass_far(key, ds):
            pass_on(key, ds)
            for d in ds:
                at = block(buf, zp(-d), y)
                send(at, at, (z, yp(2), x, c), passed, far_in)

        def near_done(key, ds):
            for sem in near_in[key]:
                wait(blocks(buf, len(ds)), sem)

        def done():
            wait(far_bytes, far_in)

        return pass_on, relay, pass_far, near_done, done

    mine = lax.rem(z, 2)

    def spread(m, buf):
        pair = buf.shape[0] == Z
        whole = buf.at[:, 0, 0]
        part_half = buf.at[pl.ds(0, buf.shape[0] // 2), 0, 0]
        all3 = buf.at[:, pl.ds(0, 3), 0] if pair else buf.at[:, 0, pl.ds(0, 3)]
        swapped, swap_in = send_group(all3), new_sem()
        ways = ((1, 0), (-1, 1))

        def piece(row, part, half=None):
            n = buf.shape[0] if half is None else buf.shape[0] // 2
            zs = pl.ds((half or 0) * n, n)
            return buf.at[zs, row, part] if pair else buf.at[zs, part, row]

        def swap_rows():
            for direction, h in ways:
                at = piece(yp(-direction), mine)
                send(at, at, (zp(direction), y, x, c), swapped, swap_in)

        def swap_far():
            for direction, h in ways:
                at = piece(yp(2), mine, h)
                send(at, at, (zp(direction), y, x, c), swapped, swap_in)

        def done():
            wait(all3, swap_in)

        if m == "ou0":
            return swap_rows, swap_far, done
        sent = send_group(buf.at[:, 0] if pair else buf.at[:, :, 0])
        passed = send_group(whole)
        row_in, far_in = [new_sem(), new_sem()], [new_sem(), new_sem()]

        def a():
            for direction, h in ways:
                send(piece(y, mine), piece(y, mine), (z, yp(direction), x, c), sent, row_in[h])

        def b():
            for direction, h in ways:
                wait(whole, row_in[h])
                at = piece(yp(-direction), mine, h)
                send(at, at, (z, yp(direction), x, c), passed, far_in[h])
            swap_rows()

        def e():
            for _, h in ways:
                wait(part_half, far_in[h])
            swap_far()

        return a, b, e, done

    def gather_tp(buf, h):
        me, other = buf.at[tp, h], (z, y, x, 1 - c)
        out = send_group(buf.at[pl.ds(0, TP - 1), h])
        near_in, far_in, mate = new_sem(), new_sem(), new_sem()

        def slot(d):
            return buf.at[xp(d) * C + 1 - c, h]

        def begin():
            for d, sem in ((2, far_in), (1, near_in), (-1, near_in)):
                send(me, me, (z, y, xp(d), 1 - c), out, sem)
            send(me, me, other, out, mate)

        def near():
            wait(buf.at[pl.ds(0, 2), h], near_in)
            for d in (1, -1):
                send(slot(d), slot(d), other, out, mate)

        def last():
            wait(me, far_in)
            send(slot(2), slot(2), other, out, mate)

        def done():
            wait(buf.at[pl.ds(0, X), h], mate)

        return begin, near, last, done

    rows_all, width = xs.shape
    cols = gx.shape[2] * 2
    nh = rows_all // 2

    def normalise(layer, h):
        n = 64
        for i in range(nh // n):
            rows = pl.ds(h * nh + i * n, n)

            def group(g):
                if layer == 0:
                    return xs[rows, pl.ds(g * 128, 128)].astype(F32)
                return s1[g % TP, h, g // TP, pl.ds(i * n, n), :].astype(F32)

            total = None
            for g in range(width // 128):
                wide = group(g)
                total = wide * wide if total is None else total + wide * wide
            scale = lax.rsqrt(jnp.sum(total, axis=1, keepdims=True) / width + EPS)
            for g in range(width // 128):
                gain = ngain[pl.ds(layer, 1), pl.ds(g * 128, 128)]
                nb[rows, pl.ds(g * 128, 128)] = (group(g) * scale * gain).astype(BF16)

    def project(layer, buf, gb, h):
        n = nb[pl.ds(h * nh, nh), :]
        value = jnp.dot(n, buf[:, :, 0].reshape(width, cols), preferred_element_type=F32)
        gate = jnp.dot(n, buf[:, :, 1].reshape(width, cols), preferred_element_type=F32)
        gated = (value * sigmoid(gate)).astype(BF16)
        if h:
            gb[...] = gated[nh - HALO :]
        wide = gated.astype(F32)
        for j in range(2):
            gx[j, HALO + h * nh : HALO + h * nh + nh, :] = wide[:, j * 128 : (j + 1) * 128]

    def convolve(layer, f, block):
        n = 64
        first = block * n + HALO - 30
        for j in range(2):
            acc = None
            for k in range(31):
                term = taps[k, pl.ds(layer, 1), pl.ds(j * 128, 128)] * gx[j, first + k : first + k + n, :]
                acc = term if acc is None else acc + term
            f[tp, block // 2, (block % 2) * n : (block % 2) * n + n, j * 128 : (j + 1) * 128] = acc.astype(BF16)

    def halo(gb, hbuf):
        copy = pltpu.make_async_remote_copy(
            src_ref=gb, dst_ref=hbuf, send_sem=new_sem(), recv_sem=new_sem(),
            device_id=after, device_id_type=MESH,
        )

        @pl.when(sp < Z * Y - 1)
        def _():
            copy.start()

        def arrives():
            @pl.when(sp > 0)
            def _():
                copy.wait_recv()
                for j in range(2):
                    gx[j, 0:HALO, :] = hbuf[:, j * 128 : (j + 1) * 128].astype(F32)

            @pl.when(sp == 0)
            def _():
                gx[:, 0:HALO, :] = jnp.zeros((2, HALO, 128), F32)

        def sent():
            @pl.when(sp < Z * Y - 1)
            def _():
                copy.wait_send()

        return arrives, sent

    def activate_and_project(layer, f, ou, nxt, h):
        first = second = jnp.zeros((nh, 128), F32)
        for k in range(TP):
            for j in range(2):
                part = f[k, h, :, j * 128 : (j + 1) * 128].astype(F32)
                first = first + part
                second = second + part * part
        mean = jnp.sum(first, axis=1, keepdims=True) / width
        var = jnp.sum(second, axis=1, keepdims=True) / width - mean * mean
        scale = lax.rsqrt(var + EPS)
        total = [jnp.zeros((nh, 128), F32) for _ in range(2)]
        for k in range(TP):
            v = (f[k, h].astype(F32) - mean) * scale * cg[k, pl.ds(layer, 1), :]
            act = (v * sigmoid(v)).astype(BF16)
            for hi in range(2):
                slot = lax.rem(tp + hi * TP + lax.rem(k - tp + 12, TP) + Z - 4, Z)
                w = ou[lax.div(slot, 2), lax.rem(slot, 2)].reshape(128, cols)
                total[hi] = total[hi] + lax.dot_general(
                    act, w, (((1,), (1,)), ((), ())), preferred_element_type=F32
                )
        for hi in range(2):
            if layer == 0:
                lane = pl.multiple_of((hi * TP + tp) * 128, 128)
                old = xs[pl.ds(h * nh, nh), pl.ds(lane, 128)]
            else:
                old = s1[tp, h, hi]
            nxt[tp, h, hi] = (old.astype(F32) + total[hi]).astype(BF16)

    perm_send = send_group(ow)
    perm_recv = new_sem()
    perm = [
        pltpu.make_async_remote_copy(
            src_ref=ow.at[layer], dst_ref=block(buf, to_z, y), send_sem=perm_send, recv_sem=perm_recv,
            device_id=goes_to, device_id_type=MESH,
        )
        for layer, buf in ((0, ou0), (1, ou1))
    ]
    drains.pop()
    stay = [pltpu.make_async_copy(ow.at[layer], block(buf, z, y), perm_recv) for layer, buf in ((0, ou0), (1, ou1))]

    def perm_start():
        @pl.when(far)
        def _():
            for copy in perm:
                copy.start()

        @pl.when(jnp.logical_not(far))
        def _():
            for copy in stay:
                copy.start()

    def perm_done():
        wait(ow, perm_recv)

    pass_vg, relay_vg, far_vg, near_vg, done_vg = y_group("vg0", vg0)
    pass_ou, relay_ou, far_ou, near_ou, done_ou = y_group("ou0", ou0)
    ou0_swap_rows, ou0_swap_far, ou0_done = spread("ou0", ou0)
    vg1_a, vg1_b, vg1_c, vg1_done = spread("vg1", vg1)
    ou1_a, ou1_b, ou1_c, ou1_done = spread("ou1", ou1)

    def vg0_stage(s):
        for part in range(2):
            if s:
                z_wait("vg0", vg0, RING, s - 1, part)
            if s < 4:
                z_stage("vg0", vg0, RING, s, part)

    wait(vg0.at[z, y], own_sem[0])
    vg0_stage(0)
    pass_vg(0, [0])
    perm_start()
    wait(vg1.at[z, y], own_sem[1])
    z_stage("vg1", vg1, RING, 0)
    wait(cg.at[tp], own_sem[3])
    gain_sent, gain_in = send_group(cg.at[pl.ds(0, TP - 1)]), new_sem()
    for d in range(1, TP):
        to = lax.rem(tp + d, TP)
        send(cg.at[tp], cg.at[tp], (z, y, lax.div(to, C), lax.rem(to, C)), gain_sent, gain_in)
    wait(xs, own_sem[2])
    with scope("norm0"):
        for h in range(2):
            normalise(0, h)

    ring = [[0]] + [brought(RING, s) for s in range(4)]

    def go_on(m, buf, plan, s):
        z_wait(m, buf, plan, s - 1)
        if s < len(plan):
            z_stage(m, buf, plan, s)

    def vg1_step(s):
        go_on("vg1", vg1, RING, s)

    def ou0_step(s):
        go_on("ou0", ou0, RING, s)

    def ou1_step(s):
        go_on("ou1", ou1, RING, s)

    even = [[d for d in ds if d % 2 == 0] for ds in ring]

    with scope("stage1"):
        vg0_stage(1)
        pass_vg(1, ring[1])
        relay_vg(0, ring[0])
        perm_done()
        z_stage("ou0", ou0, RING, 0)
        pass_ou(0, even[0])
    with scope("stage2"):
        vg0_stage(2)
        pass_vg(2, ring[2])
        relay_vg(1, ring[1])
        ou0_step(1)
        pass_ou(1, even[1])
        vg1_step(1)
    with scope("stage3"):
        vg0_stage(3)
        pass_vg(3, ring[3])
        relay_vg(2, ring[2])
        ou0_step(2)
        pass_ou(2, even[2])
        relay_ou(0, even[0])
        vg1_step(2)
    with scope("stage4"):
        vg0_stage(4)
        far_vg(4, ring[4])
        relay_vg(3, ring[3])
        ou0_step(3)
        pass_ou(3, even[3])
        relay_ou(1, even[1])
        vg1_step(3)
        z_stage("ou1", ou1, RING, 0)
    with scope("vg0done"):
        near_vg(4, ring[4])
        done_vg()

    def layer_head(layer, vg, gb, hbuf, f, ready, hook):
        first, second = gather_tp(f, 1), gather_tp(f, 0)
        with scope("proj"):
            project(layer, vg, gb, 1)
        arrives, sent = halo(gb, hbuf)
        with scope("hookp"):
            hook()
        with scope("projb"):
            ready()
            project(layer, vg, gb, 0)
        with scope("conv"):
            convolve(layer, f, 2)
            convolve(layer, f, 3)
        first[0]()
        with scope("convb"):
            convolve(layer, f, 1)
        return first, second, arrives, sent

    def layer_tail(layer, f, ou, nxt, parts, arrives, hooks):
        first, second = parts
        with scope("hook0"):
            hooks[0]()
        with scope("halo"):
            arrives()
            convolve(layer, f, 0)
        second[0]()
        with scope("hook0b"):
            hooks[1]()
        with scope("ag1"):
            first[1]()
            first[2]()
        with scope("hook1"):
            hooks[2]()
        with scope("ag1b"):
            first[3]()
        with scope("hook2"):
            hooks[3]()
        first2, second2 = gather_tp(nxt, 1), gather_tp(nxt, 0)
        with scope("act"):
            activate_and_project(layer, f, ou, nxt, 1)
        first2[0]()
        with scope("ag1c"):
            for step in second[1:]:
                step()
        with scope("actb"):
            activate_and_project(layer, f, ou, nxt, 0)
        second2[0]()
        with scope("hook3"):
            hooks[4]()
        with scope("ag2"):
            first2[1]()
            first2[2]()
        with scope("hook4"):
            hooks[5]()
        with scope("ag2b"):
            first2[3]()
        return second2

    def nothing():
        pass

    def hook0p():
        ou0_step(4)
        far_ou(4, even[4])
        relay_ou(2, even[2])
        relay_ou(3, even[3])
        ou1_step(1)

    first, second, arrives, sent0 = layer_head(0, vg0, gb0, h0, f0, nothing, hook0p)

    def hook00():
        vg1_step(4)
        vg1_a()

    def hook00b():
        near_ou(4, even[4])
        ou0_swap_rows()
        ou1_step(2)

    def hook01():
        done_ou()
        ou0_swap_far()
        ou1_step(3)

    def hook02():
        vg1_b()
        wait(cg.at[pl.ds(0, TP - 1)], gain_in)
        ou0_done()

    def hook03():
        ou1_step(4)

    def hook04():
        vg1_c()
        ou1_a()

    rest = layer_tail(
        0, f0, ou0, s1, (first, second), arrives, (hook00, hook00b, hook01, hook02, hook03, hook04)
    )
    with scope("norm1"):
        normalise(1, 1)

    def ready():
        with scope("ag2c"):
            for step in rest[1:]:
                step()
        normalise(1, 0)

    with scope("vg1done"):
        ou1_b()
        vg1_done()

    first, second, arrives, sent1 = layer_head(1, vg1, gb1, h1, f1, ready, nothing)
    rest1 = layer_tail(
        1, f1, ou1, s2, (first, second), arrives, (nothing, ou1_c, nothing, ou1_done, nothing, nothing)
    )

    def write(h):
        for g in range(width // 128):
            out_ref[h * nh : (h + 1) * nh, g * 128 : (g + 1) * 128] = s2[g % TP, h, g // TP]

    write(1)
    with scope("ag2c"):
        for step in rest1[1:]:
            step()
    write(0)

    with scope("out"):
        for ref, sem in drains:
            wait(ref, sem)
        sent0()
        sent1()

        @pl.when(far)
        def _():
            wait(ow, perm_send)

    assert used[0] == N_SEMS, used[0]


def body(stream_in, norm_gain, value_weight, gate_weight, conv_taps, channel_gain, out_weight):
    rows, width = stream_in.shape
    depth, cols = value_weight.shape[1:]
    hbm, vmem = pl.BlockSpec(memory_space=pltpu.HBM), pl.BlockSpec(memory_space=pltpu.VMEM)
    out_t = jnp.swapaxes(out_weight, 1, 2)
    taps = jnp.swapaxes(conv_taps, 0, 1)
    return pl.pallas_call(
        kernel,
        out_shape=pltpu.VMEM((rows, width), BF16),
        in_specs=[hbm, vmem, hbm, hbm, vmem, hbm, hbm],
        out_specs=vmem,
        scratch_shapes=[
            pltpu.VMEM((Z, Y, 2, depth, cols), BF16),
            pltpu.VMEM((Z, Y, 2, depth, cols), BF16),
            pltpu.VMEM((Z // 2, 2, Y, depth, cols), BF16),
            pltpu.VMEM((Z // 2, 2, Y, depth, cols), BF16),
            pltpu.VMEM((rows, width), BF16),
            pltpu.VMEM((TP, 2, 2, rows // 2, 128), BF16),
            pltpu.VMEM((TP, 2, 2, rows // 2, 128), BF16),
            pltpu.VMEM((TP, 2, rows // 2, cols), BF16),
            pltpu.VMEM((TP, 2, rows // 2, cols), BF16),
            pltpu.VMEM((rows, width), BF16),
            pltpu.VMEM((2, rows + HALO, 128), F32),
            pltpu.VMEM((HALO, cols), BF16),
            pltpu.VMEM((HALO, cols), BF16),
            pltpu.VMEM((HALO, cols), BF16),
            pltpu.VMEM((HALO, cols), BF16),
            pltpu.VMEM((TP, 2, cols), F32),
            pltpu.SemaphoreType.DMA((N_SEMS,)),
        ],
        compiler_params=pltpu.CompilerParams(
            collective_id=0, has_side_effects=True, vmem_limit_bytes=VMEM_LIMIT
        ),
    )(stream_in, norm_gain, value_weight, gate_weight, taps, channel_gain, out_t)


def solution(mesh):
    finer = Mesh(mesh.devices.reshape(Z, Y, X, C), ("z", "y", "x", "c"))
    sp, tp = ("z", "y"), ("x", "c")
    placed = (
        P(sp, None),
        P(),
        P(None, sp, tp),
        P(None, sp, tp),
        P(None, None, tp),
        P(None, tp),
        P(None, tp, sp),
    )
    return jax.shard_map(body, mesh=finer, in_specs=placed, out_specs=P(sp, None), check_vma=False)
```

```python
import jax
import jax.numpy as jnp
from jax import lax
from jax.experimental import pallas as pl
from jax.experimental.pallas import tpu as pltpu
from jax.sharding import Mesh
from jax.sharding import PartitionSpec as P

Z, Y, X, C = 16, 4, 4, 2
TP = X * C
MESH = pl.DeviceIdType.MESH
EPS = 1e-05
F32 = jnp.float32
BF16 = jnp.bfloat16
N_SEMS = 143
HALO = 32
RING = [
    [(2 * s, tuple(d for d in (2 * s + 2, 2 * s + 1) if d <= Z // 2)),
     (-2 * s, tuple(-d for d in (2 * s + 2, 2 * s + 1) if d < Z // 2))]
    for s in range(4)
]
VMEM_LIMIT = 60_000_000
CHUNKS = 4
scope = jax.named_scope


def sigmoid(v):
    return 0.5 + 0.5 * jnp.tanh(0.5 * v)


def kernel(
    stream_hbm, ngain_hbm, vw, gw, taps_hbm, cgain, ow, out_ref,
    taps, ngain, vg0, vg1, ou0, ou1, xs, s1, s2, f0, f1, nb, gx, h0, h1, gb0, gb1, cg, sems,
):
    z, y, x, c = (lax.axis_index(a) for a in ("z", "y", "x", "c"))
    tp = x * C + c
    sp = z * Y + y
    used = [0]

    def new_sem():
        used[0] += 1
        return sems.at[used[0] - 1]

    def send(src, dst, device, send_sem, recv_sem):
        pltpu.make_async_remote_copy(
            src_ref=src, dst_ref=dst, send_sem=send_sem, recv_sem=recv_sem,
            device_id=device, device_id_type=MESH,
        ).start()

    def wait(ref, sem):
        pltpu.make_async_copy(ref, ref, sem).wait()

    drains = []

    def send_group(ref):
        sem = new_sem()
        drains.append((ref, sem))
        return sem

    def zp(d):
        return lax.rem(z + d + Z, Z)

    def yp(d):
        return lax.rem(y + d + Y, Y)

    def xp(d):
        return lax.rem(x + d + X, X)

    own_sem = [new_sem() for _ in range(6)]
    own = [
        pltpu.make_async_copy(vw.at[0], vg0.at[z, y, 0], own_sem[0]),
        pltpu.make_async_copy(gw.at[0], vg0.at[z, y, 1], own_sem[0]),
        pltpu.make_async_copy(vw.at[1], vg1.at[z, y, 0], own_sem[1]),
        pltpu.make_async_copy(gw.at[1], vg1.at[z, y, 1], own_sem[1]),
        pltpu.make_async_copy(stream_hbm, xs, own_sem[2]),
        pltpu.make_async_copy(cgain, cg.at[tp], own_sem[3]),
        pltpu.make_async_copy(ngain_hbm, ngain, own_sem[4]),
        pltpu.make_async_copy(taps_hbm, taps, own_sem[5]),
    ]
    for copy in own:
        copy.start()

    zlo = lax.rem(z, TP)
    far = zlo != tp
    to_z = zp(lax.rem(tp - zlo + 12, TP) - 4)
    from_z = zp(4 - lax.rem(zlo - tp + 12, TP))
    goes_to = (to_z, y, lax.div(zlo, C), lax.rem(zlo, C))
    comes_from = (from_z, y, lax.div(zlo, C), lax.rem(zlo, C))
    nsp = lax.rem(sp + 1, Z * Y)
    psp = lax.rem(sp + Z * Y - 1, Z * Y)
    after = (lax.div(nsp, Y), lax.rem(nsp, Y), x, c)
    before = (lax.div(psp, Y), lax.rem(psp, Y), x, c)

    barrier = pltpu.get_barrier_semaphore()
    peers = [(zp(d), y, x, c) for d in (1, 2, -1, -2)] + [(z, yp(d), x, c) for d in (1, -1, 2)]
    for d in range(1, TP):
        other = lax.rem(tp + d, TP)
        peers.append((z, y, lax.div(other, C), lax.rem(other, C)))
    peers += [after, before]
    for peer in peers:
        pl.semaphore_signal(barrier, inc=1, device_id=peer, device_id_type=MESH)

    @pl.when(far)
    def _():
        pl.semaphore_signal(barrier, inc=1, device_id=comes_from, device_id_type=MESH)

    with scope("barrier"):
        pl.semaphore_wait(barrier, len(peers) + jnp.where(far, 1, 0))

    def block(buf, slot, row, part=None):
        if buf.shape[0] != Z:
            return buf.at[lax.div(slot, 2), lax.rem(slot, 2), row]
        return buf.at[slot, row] if part is None else buf.at[slot, row, part]

    def blocks(buf, n, part=None):
        if buf.shape[0] != Z:
            return buf.at[pl.ds(0, max(1, n // 3)), 0, pl.ds(0, 3)] if n % 3 == 0 else buf.at[pl.ds(0, 1), 0, pl.ds(0, n)]
        return buf.at[pl.ds(0, n), 0] if part is None else buf.at[pl.ds(0, n), 0, part]

    z_sems = {}

    def brought(plan, s):
        return [d for _, news in plan[s] for d in news]

    def z_stage(m, buf, plan, s, part=None):
        if s == 0:
            z_sems[m, part] = [new_sem() for _ in plan], send_group(blocks(buf, Z - 1, part))
        sems_in, out = z_sems[m, part]
        for d, news in plan[s]:
            at = block(buf, zp(-d), y, part)
            for new in news:
                send(at, at, (zp(new - d), y, x, c), out, sems_in[s])

    def z_wait(m, buf, plan, s, part=None):
        wait(blocks(buf, len(brought(plan, s)), part), z_sems[m, part][0][s])

    def y_group(m, buf):
        pair = buf.shape[0] == Z
        sent = send_group(buf.at[:, pl.ds(0, 2)] if pair else buf.at[pl.ds(0, 4), 0])
        far_bytes = buf.at[:, 0] if pair else buf.at[pl.ds(0, 2), 0]
        passed, far_in, near_in = send_group(far_bytes), new_sem(), {}

        def half(slot, row, h):
            return buf.at[slot, row, h] if pair else block(buf, slot, row).at[pl.ds(h * 16, 16)]

        def pass_on(key, ds):
            near_in[key] = new_sem(), new_sem()
            for d in ds:
                at = block(buf, zp(-d), y)
                for direction, sem in zip((1, -1), near_in[key]):
                    send(at, at, (z, yp(direction), x, c), sent, sem)

        def relay(key, ds):
            for direction, h in ((1, 0), (-1, 1)):
                wait(blocks(buf, len(ds)), near_in[key][h])
                for d in ds:
                    at = half(zp(-d), yp(-direction), h)
                    send(at, at, (z, yp(direction), x, c), passed, far_in)

        def pass_far(key, ds):
            pass_on(key, ds)
            for d in ds:
                at = block(buf, zp(-d), y)
                send(at, at, (z, yp(2), x, c), passed, far_in)

        def near_done(key, ds):
            for sem in near_in[key]:
                wait(blocks(buf, len(ds)), sem)

        def done():
            wait(far_bytes, far_in)

        return pass_on, relay, pass_far, near_done, done

    mine = lax.rem(z, 2)

    def spread(m, buf, first=0, count=None):
        pair = buf.shape[0] == Z
        count = count or buf.shape[0]
        some = pl.ds(first, count)
        whole = buf.at[some, 0, 0]
        part_half = buf.at[pl.ds(first, count // 2), 0, 0]
        all3 = buf.at[some, pl.ds(0, 3), 0] if pair else buf.at[some, 0, pl.ds(0, 3)]
        swapped, swap_in = send_group(all3), new_sem()
        ways = ((1, 0), (-1, 1))

        def piece(row, part, half=None):
            n = count if half is None else count // 2
            zs = pl.ds(first + (half or 0) * n, n)
            return buf.at[zs, row, part] if pair else buf.at[zs, part, row]

        def swap_rows():
            for direction, h in ways:
                at = piece(yp(-direction), mine)
                send(at, at, (zp(direction), y, x, c), swapped, swap_in)

        def swap_far():
            for direction, h in ways:
                at = piece(yp(2), mine, h)
                send(at, at, (zp(direction), y, x, c), swapped, swap_in)

        def done():
            wait(all3, swap_in)

        if m == "ou0":
            return swap_rows, swap_far, done
        sent = send_group(buf.at[some, 0] if pair else buf.at[some, :, 0])
        passed = send_group(whole)
        row_in, far_in = [new_sem(), new_sem()], [new_sem(), new_sem()]

        def a():
            for direction, h in ways:
                send(piece(y, mine), piece(y, mine), (z, yp(direction), x, c), sent, row_in[h])

        def b():
            for direction, h in ways:
                wait(whole, row_in[h])
                at = piece(yp(-direction), mine, h)
                send(at, at, (z, yp(direction), x, c), passed, far_in[h])
            swap_rows()

        def e():
            for _, h in ways:
                wait(part_half, far_in[h])
            swap_far()

        return a, b, e, done

    def gather_tp(buf):
        out = send_group(buf.at[pl.ds(0, TP - 1)])
        return [gather_chunk(buf, h, out) for h in range(CHUNKS)]

    def gather_chunk(buf, h, out):
        me, other = buf.at[tp, h], (z, y, x, 1 - c)
        near_in, far_in, mate = new_sem(), new_sem(), new_sem()

        def slot(d):
            return buf.at[xp(d) * C + 1 - c, h]

        def begin():
            for d, sem in ((2, far_in), (1, near_in), (-1, near_in)):
                send(me, me, (z, y, xp(d), 1 - c), out, sem)
            send(me, me, other, out, mate)

        def near():
            wait(buf.at[pl.ds(0, 2), h], near_in)
            for d in (1, -1):
                send(slot(d), slot(d), other, out, mate)

        def far_one():
            wait(me, far_in)
            send(slot(2), slot(2), other, out, mate)

        def done():
            wait(buf.at[pl.ds(0, X), h], mate)

        return begin, near, far_one, done

    rows_all, width = xs.shape
    cols = gx.shape[2] * 2
    nh = rows_all // CHUNKS
    last = CHUNKS - 1

    def normalise(layer, h):
        rows = pl.ds(h * nh, nh)

        def group(g):
            if layer == 0:
                return xs[rows, pl.ds(g * 128, 128)].astype(F32)
            return s1[g % TP, h, g // TP].astype(F32)

        total = None
        for g in range(width // 128):
            wide = group(g)
            total = wide * wide if total is None else total + wide * wide
        scale = lax.rsqrt(jnp.sum(total, axis=1, keepdims=True) / width + EPS)
        for g in range(width // 128):
            gain = ngain[pl.ds(layer, 1), pl.ds(g * 128, 128)]
            nb[rows, pl.ds(g * 128, 128)] = (group(g) * scale * gain).astype(BF16)

    def project(layer, buf, gb, h):
        n = nb[pl.ds(h * nh, nh), :]
        value = jnp.dot(n, buf[:, :, 0].reshape(width, cols), preferred_element_type=F32)
        gate = jnp.dot(n, buf[:, :, 1].reshape(width, cols), preferred_element_type=F32)
        gated = (value * sigmoid(gate)).astype(BF16)
        if h == last:
            gb[...] = gated[nh - HALO :]
        wide = gated.astype(F32)
        for j in range(2):
            gx[j, HALO + h * nh : HALO + h * nh + nh, :] = wide[:, j * 128 : (j + 1) * 128]

    def convolve(layer, f, h):
        first = h * nh + HALO - 30
        for j in range(2):
            acc = None
            for k in range(31):
                term = taps[k, pl.ds(layer, 1), pl.ds(j * 128, 128)] * gx[j, first + k : first + k + nh, :]
                acc = term if acc is None else acc + term
            f[tp, h, :, j * 128 : (j + 1) * 128] = acc.astype(BF16)

    def halo(gb, hbuf):
        copy = pltpu.make_async_remote_copy(
            src_ref=gb, dst_ref=hbuf, send_sem=new_sem(), recv_sem=new_sem(),
            device_id=after, device_id_type=MESH,
        )

        @pl.when(sp < Z * Y - 1)
        def _():
            copy.start()

        def arrives():
            @pl.when(sp > 0)
            def _():
                copy.wait_recv()
                for j in range(2):
                    gx[j, 0:HALO, :] = hbuf[:, j * 128 : (j + 1) * 128].astype(F32)

            @pl.when(sp == 0)
            def _():
                gx[:, 0:HALO, :] = jnp.zeros((2, HALO, 128), F32)

        def sent():
            @pl.when(sp < Z * Y - 1)
            def _():
                copy.wait_send()

        return arrives, sent

    def activate_and_project(layer, f, ou, nxt, h):
        first = second = jnp.zeros((nh, 128), F32)
        for k in range(TP):
            for j in range(2):
                part = f[k, h, :, j * 128 : (j + 1) * 128].astype(F32)
                first = first + part
                second = second + part * part
        mean = jnp.sum(first, axis=1, keepdims=True) / width
        var = jnp.sum(second, axis=1, keepdims=True) / width - mean * mean
        scale = lax.rsqrt(var + EPS)
        total = [jnp.zeros((nh, 128), F32) for _ in range(2)]
        for k in range(TP):
            v = (f[k, h].astype(F32) - mean) * scale * cg[k, pl.ds(layer, 1), :]
            act = (v * sigmoid(v)).astype(BF16)
            for hi in range(2):
                slot = lax.rem(tp + hi * TP + lax.rem(k - tp + 12, TP) + Z - 4, Z)
                w = ou[lax.div(slot, 2), lax.rem(slot, 2)].reshape(128, cols)
                total[hi] = total[hi] + lax.dot_general(
                    act, w, (((1,), (1,)), ((), ())), preferred_element_type=F32
                )
        for hi in range(2):
            if layer == 0:
                lane = pl.multiple_of((hi * TP + tp) * 128, 128)
                old = xs[pl.ds(h * nh, nh), pl.ds(lane, 128)]
            else:
                old = s1[tp, h, hi]
            nxt[tp, h, hi] = (old.astype(F32) + total[hi]).astype(BF16)

    perm_send = send_group(ow)
    perm_recv = new_sem()
    perm = [
        pltpu.make_async_remote_copy(
            src_ref=ow.at[layer], dst_ref=block(buf, to_z, y), send_sem=perm_send, recv_sem=perm_recv,
            device_id=goes_to, device_id_type=MESH,
        )
        for layer, buf in ((0, ou0), (1, ou1))
    ]
    drains.pop()
    stay = [pltpu.make_async_copy(ow.at[layer], block(buf, z, y), perm_recv) for layer, buf in ((0, ou0), (1, ou1))]

    def perm_start():
        @pl.when(far)
        def _():
            for copy in perm:
                copy.start()

        @pl.when(jnp.logical_not(far))
        def _():
            for copy in stay:
                copy.start()

    def perm_done():
        wait(ow, perm_recv)

    pass_vg, relay_vg, far_vg, near_vg, done_vg = y_group("vg0", vg0)
    pass_ou, relay_ou, far_ou, near_ou, done_ou = y_group("ou0", ou0)
    ou0_swap_rows, ou0_swap_far, ou0_done = spread("ou0", ou0)
    vg1_a, vg1_b, vg1_c, vg1_done = zip(*(spread("vg1", vg1, n, Z // 2) for n in (0, Z // 2)))
    ou1_a, ou1_b, ou1_c, ou1_done = spread("ou1", ou1)

    def vg0_stage(s):
        for part in range(2):
            if s:
                z_wait("vg0", vg0, RING, s - 1, part)
            if s < 4:
                z_stage("vg0", vg0, RING, s, part)

    wait(vg0.at[z, y], own_sem[0])
    vg0_stage(0)
    pass_vg(0, [0])
    perm_start()
    wait(vg1.at[z, y], own_sem[1])
    z_stage("vg1", vg1, RING, 0)
    wait(cg.at[tp], own_sem[3])
    gain_sent, gain_in = send_group(cg.at[pl.ds(0, TP - 1)]), new_sem()
    for d in range(1, TP):
        to = lax.rem(tp + d, TP)
        send(cg.at[tp], cg.at[tp], (z, y, lax.div(to, C), lax.rem(to, C)), gain_sent, gain_in)
    wait(xs, own_sem[2])
    wait(ngain, own_sem[4])
    with scope("norm0"):
        for h in range(CHUNKS):
            normalise(0, h)

    ring = [[0]] + [brought(RING, s) for s in range(4)]

    def go_on(m, buf, plan, s):
        z_wait(m, buf, plan, s - 1)
        if s < len(plan):
            z_stage(m, buf, plan, s)

    def vg1_step(s):
        go_on("vg1", vg1, RING, s)

    def ou0_step(s):
        go_on("ou0", ou0, RING, s)

    def ou1_step(s):
        go_on("ou1", ou1, RING, s)

    even = [[d for d in ds if d % 2 == 0] for ds in ring]

    with scope("stage1"):
        vg0_stage(1)
        pass_vg(1, ring[1])
        relay_vg(0, ring[0])
        perm_done()
        z_stage("ou0", ou0, RING, 0)
        pass_ou(0, even[0])
    with scope("stage2"):
        vg0_stage(2)
        pass_vg(2, ring[2])
        relay_vg(1, ring[1])
        ou0_step(1)
        pass_ou(1, even[1])
        vg1_step(1)
    with scope("stage3"):
        vg0_stage(3)
        pass_vg(3, ring[3])
        relay_vg(2, ring[2])
        ou0_step(2)
        pass_ou(2, even[2])
        relay_ou(0, even[0])
        vg1_step(2)
    with scope("stage4"):
        vg0_stage(4)
        far_vg(4, ring[4])
        relay_vg(3, ring[3])
        ou0_step(3)
        pass_ou(3, even[3])
        relay_ou(1, even[1])
        vg1_step(3)
        z_stage("ou1", ou1, RING, 0)
    wait(taps, own_sem[5])
    with scope("vg0done"):
        near_vg(4, ring[4])
        done_vg()

    order = range(CHUNKS - 1, -1, -1)

    def receive(gather, h, between=None):
        if h == last:
            gather[h][1]()
            gather[h][2]()
            if between:
                between()
        if h:
            gather[h - 1][1]()
            gather[h - 1][2]()
        gather[h][3]()

    def layer_of(layer, vg, gb, hbuf, f, ou, nxt, source, weights_ready, hooks):
        first, second = gather_tp(f), gather_tp(nxt)

        def hook(name):
            if name in hooks:
                with scope(name):
                    hooks[name]()

        for h in order:
            if source is not None:
                with scope("get%d" % h):
                    receive(source, h)
                normalise(layer, h)
            if h == last:
                weights_ready()
            with scope("proj%d" % h):
                project(layer, vg, gb, h)
            if h == last:
                arrives, sent = halo(gb, hbuf)
                hook("hookp")
            else:
                convolve(layer, f, h + 1)
                first[h + 1][0]()
                hook("head%d" % h)
        hook("hook0")
        with scope("halo"):
            arrives()
            convolve(layer, f, 0)
        first[0][0]()
        hook("hook0b")
        for h in order:
            with scope("ag%d" % h):
                receive(first, h, lambda: hook("hook1"))
            if h == last:
                hook("hook2")
            with scope("act%d" % h):
                activate_and_project(layer, f, ou, nxt, h)
            second[h][0]()
            hook("after%d" % h)
        return second, sent

    def hook0p():
        ou0_step(4)
        far_ou(4, even[4])
        relay_ou(2, even[2])
        relay_ou(3, even[3])
        ou1_step(1)

    def hook00():
        vg1_step(4)
        vg1_a[0]()

    def hook00b():
        near_ou(4, even[4])
        ou0_swap_rows()
        vg1_a[1]()
        ou1_step(2)

    def hook01():
        done_ou()
        ou0_swap_far()
        vg1_b[0]()
        ou1_step(3)

    def hook02():
        vg1_b[1]()
        wait(cg.at[pl.ds(0, TP - 1)], gain_in)
        ou0_done()

    def hook03():
        ou1_step(4)
        ou1_a()

    hooks0 = {
        "hookp": hook0p, "hook0": hook00, "hook0b": hook00b, "hook1": hook01, "hook2": hook02,
        "after3": vg1_c[0], "after2": vg1_c[1], "after1": hook03,
    }
    rest, sent0 = layer_of(0, vg0, gb0, h0, f0, ou0, s1, None, lambda: None, hooks0)

    def ready():
        with scope("vg1done"):
            ou1_b()
            vg1_done[0]()
            vg1_done[1]()

    hooks1 = {"head1": ou1_c, "hook2": ou1_done}
    rest1, sent1 = layer_of(1, vg1, gb1, h1, f1, ou1, s2, rest, ready, hooks1)
    for h in order:
        with scope("last%d" % h):
            receive(rest1, h)
        for g in range(width // 128):
            out_ref[h * nh : (h + 1) * nh, g * 128 : (g + 1) * 128] = s2[g % TP, h, g // TP]

    with scope("out"):
        for ref, sem in drains:
            wait(ref, sem)
        sent0()
        sent1()

        @pl.when(far)
        def _():
            wait(ow, perm_send)

    assert used[0] == N_SEMS, used[0]


def body(stream_in, norm_gain, value_weight, gate_weight, conv_taps, channel_gain, out_weight):
    rows, width = stream_in.shape
    depth, cols = value_weight.shape[1:]
    hbm, vmem = pl.BlockSpec(memory_space=pltpu.HBM), pl.BlockSpec(memory_space=pltpu.VMEM)
    out_t = jnp.swapaxes(out_weight, 1, 2)
    taps = jnp.swapaxes(conv_taps, 0, 1)
    return pl.pallas_call(
        kernel,
        out_shape=pltpu.VMEM((rows, width), BF16),
        in_specs=[hbm] * 7,
        out_specs=vmem,
        scratch_shapes=[
            pltpu.VMEM(taps.shape, F32),
            pltpu.VMEM(norm_gain.shape, F32),
            pltpu.VMEM((Z, Y, 2, depth, cols), BF16),
            pltpu.VMEM((Z, Y, 2, depth, cols), BF16),
            pltpu.VMEM((Z // 2, 2, Y, depth, cols), BF16),
            pltpu.VMEM((Z // 2, 2, Y, depth, cols), BF16),
            pltpu.VMEM((rows, width), BF16),
            pltpu.VMEM((TP, CHUNKS, 2, rows // CHUNKS, 128), BF16),
            pltpu.VMEM((TP, CHUNKS, 2, rows // CHUNKS, 128), BF16),
            pltpu.VMEM((TP, CHUNKS, rows // CHUNKS, cols), BF16),
            pltpu.VMEM((TP, CHUNKS, rows // CHUNKS, cols), BF16),
            pltpu.VMEM((rows, width), BF16),
            pltpu.VMEM((2, rows + HALO, 128), F32),
            pltpu.VMEM((HALO, cols), BF16),
            pltpu.VMEM((HALO, cols), BF16),
            pltpu.VMEM((HALO, cols), BF16),
            pltpu.VMEM((HALO, cols), BF16),
            pltpu.VMEM((TP, 2, cols), F32),
            pltpu.SemaphoreType.DMA((N_SEMS,)),
        ],
        compiler_params=pltpu.CompilerParams(
            collective_id=0, has_side_effects=True, vmem_limit_bytes=VMEM_LIMIT
        ),
    )(stream_in, norm_gain, value_weight, gate_weight, taps, channel_gain, out_t)


def solution(mesh):
    finer = Mesh(mesh.devices.reshape(Z, Y, X, C), ("z", "y", "x", "c"))
    sp, tp = ("z", "y"), ("x", "c")
    placed = (
        P(sp, None),
        P(),
        P(None, sp, tp),
        P(None, sp, tp),
        P(None, None, tp),
        P(None, tp),
        P(None, tp, sp),
    )
    return jax.shard_map(body, mesh=finer, in_specs=placed, out_specs=P(sp, None), check_vma=False)
```

```python
import jax
import jax.numpy as jnp
from jax import lax
from jax.experimental import pallas as pl
from jax.experimental.pallas import tpu as pltpu
from jax.sharding import Mesh
from jax.sharding import PartitionSpec as P

Z, Y, X, C = 16, 4, 4, 2
TP = X * C
MESH = pl.DeviceIdType.MESH
EPS = 1e-05
F32 = jnp.float32
BF16 = jnp.bfloat16
N_SEMS = 106
HALO = 32
RING = [
    [(2 * s, tuple(d for d in (2 * s + 2, 2 * s + 1) if d <= Z // 2)),
     (-2 * s, tuple(-d for d in (2 * s + 2, 2 * s + 1) if d < Z // 2))]
    for s in range(4)
]
VMEM_LIMIT = 60_000_000
CHUNKS = 4
scope = jax.named_scope


def sigmoid(v):
    return 0.5 + 0.5 * jnp.tanh(0.5 * v)


def kernel(
    stream_hbm, ngain_hbm, vw, gw, taps_hbm, cgain, ow, out_ref,
    taps, ngain, vg0, vg1, ou0, ou1, xs, s1, s2, f0, f1, nb, gx, h0, h1, gb0, gb1, cg, sems,
):
    z, y, x, c = (lax.axis_index(a) for a in ("z", "y", "x", "c"))
    tp = x * C + c
    sp = z * Y + y
    used = [0]

    def new_sem():
        used[0] += 1
        return sems.at[used[0] - 1]

    def send(src, dst, device, send_sem, recv_sem):
        pltpu.make_async_remote_copy(
            src_ref=src, dst_ref=dst, send_sem=send_sem, recv_sem=recv_sem,
            device_id=device, device_id_type=MESH,
        ).start()

    def wait(ref, sem):
        pltpu.make_async_copy(ref, ref, sem).wait()

    drains = []

    def send_group(ref):
        sem = new_sem()
        drains.append((ref, sem))
        return sem

    def zp(d):
        return lax.rem(z + d + Z, Z)

    def yp(d):
        return lax.rem(y + d + Y, Y)

    def xp(d):
        return lax.rem(x + d + X, X)

    own_sem = [new_sem() for _ in range(6)]
    own = [
        pltpu.make_async_copy(vw.at[0], vg0.at[z, y, 0], own_sem[0]),
        pltpu.make_async_copy(gw.at[0], vg0.at[z, y, 1], own_sem[0]),
        pltpu.make_async_copy(vw.at[1], vg1.at[z, y, 0], own_sem[1]),
        pltpu.make_async_copy(gw.at[1], vg1.at[z, y, 1], own_sem[1]),
        pltpu.make_async_copy(stream_hbm, xs, own_sem[2]),
        pltpu.make_async_copy(cgain, cg.at[tp], own_sem[3]),
        pltpu.make_async_copy(ngain_hbm, ngain, own_sem[4]),
        pltpu.make_async_copy(taps_hbm, taps, own_sem[5]),
    ]
    for copy in own:
        copy.start()

    zlo = lax.rem(z, TP)
    far = zlo != tp
    to_z = zp(lax.rem(tp - zlo + 12, TP) - 4)
    from_z = zp(4 - lax.rem(zlo - tp + 12, TP))
    goes_to = (to_z, y, lax.div(zlo, C), lax.rem(zlo, C))
    comes_from = (from_z, y, lax.div(zlo, C), lax.rem(zlo, C))
    nsp = lax.rem(sp + 1, Z * Y)
    psp = lax.rem(sp + Z * Y - 1, Z * Y)
    after = (lax.div(nsp, Y), lax.rem(nsp, Y), x, c)
    before = (lax.div(psp, Y), lax.rem(psp, Y), x, c)

    barrier = pltpu.get_barrier_semaphore()
    peers = [(zp(d), y, x, c) for d in (1, 2, -1, -2)] + [(z, yp(d), x, c) for d in (1, -1, 2)]
    for d in range(1, TP):
        other = lax.rem(tp + d, TP)
        peers.append((z, y, lax.div(other, C), lax.rem(other, C)))
    peers += [after, before]
    for peer in peers:
        pl.semaphore_signal(barrier, inc=1, device_id=peer, device_id_type=MESH)

    @pl.when(far)
    def _():
        pl.semaphore_signal(barrier, inc=1, device_id=comes_from, device_id_type=MESH)

    with scope("barrier"):
        pl.semaphore_wait(barrier, len(peers) + jnp.where(far, 1, 0))

    def block(buf, slot, row, part=None):
        if buf.shape[0] != Z:
            return buf.at[lax.div(slot, 2), lax.rem(slot, 2), row]
        return buf.at[slot, row] if part is None else buf.at[slot, row, part]

    def blocks(buf, n, part=None):
        if buf.shape[0] != Z:
            return buf.at[pl.ds(0, max(1, n // 3)), 0, pl.ds(0, 3)] if n % 3 == 0 else buf.at[pl.ds(0, 1), 0, pl.ds(0, n)]
        return buf.at[pl.ds(0, n), 0] if part is None else buf.at[pl.ds(0, n), 0, part]

    z_sems = {}

    def brought(plan, s):
        return [d for _, news in plan[s] for d in news]

    def z_stage(m, buf, plan, s, part=None):
        if s == 0:
            z_sems[m, part] = [new_sem() for _ in plan], send_group(blocks(buf, Z - 1, part))
        sems_in, out = z_sems[m, part]
        for d, news in plan[s]:
            at = block(buf, zp(-d), y, part)
            for new in news:
                send(at, at, (zp(new - d), y, x, c), out, sems_in[s])

    def z_wait(m, buf, plan, s, part=None):
        wait(blocks(buf, len(brought(plan, s)), part), z_sems[m, part][0][s])

    def y_group(m, buf):
        pair = buf.shape[0] == Z
        sent = send_group(buf.at[:, pl.ds(0, 2)] if pair else buf.at[pl.ds(0, 4), 0])
        far_bytes = buf.at[:, 0] if pair else buf.at[pl.ds(0, 2), 0]
        passed, far_in, near_in = send_group(far_bytes), new_sem(), {}

        def half(slot, row, h):
            return buf.at[slot, row, h] if pair else block(buf, slot, row).at[pl.ds(h * 16, 16)]

        def pass_on(key, ds):
            near_in[key] = new_sem(), new_sem()
            for d in ds:
                at = block(buf, zp(-d), y)
                for direction, sem in zip((1, -1), near_in[key]):
                    send(at, at, (z, yp(direction), x, c), sent, sem)

        def relay(key, ds):
            for direction, h in ((1, 0), (-1, 1)):
                wait(blocks(buf, len(ds)), near_in[key][h])
                for d in ds:
                    at = half(zp(-d), yp(-direction), h)
                    send(at, at, (z, yp(direction), x, c), passed, far_in)

        def pass_far(key, ds):
            pass_on(key, ds)
            for d in ds:
                at = block(buf, zp(-d), y)
                send(at, at, (z, yp(2), x, c), passed, far_in)

        def near_done(key, ds):
            for sem in near_in[key]:
                wait(blocks(buf, len(ds)), sem)

        def done():
            wait(far_bytes, far_in)

        return pass_on, relay, pass_far, near_done, done

    mine = lax.rem(z, 2)

    def spread(m, buf, first=0, count=None):
        pair = buf.shape[0] == Z
        count = count or buf.shape[0]
        some = pl.ds(first, count)
        whole = buf.at[some, 0, 0]
        part_half = buf.at[pl.ds(first, count // 2), 0, 0]
        all3 = buf.at[some, pl.ds(0, 3), 0] if pair else buf.at[some, 0, pl.ds(0, 3)]
        swapped, swap_in = send_group(all3), new_sem()
        ways = ((1, 0), (-1, 1))

        def piece(row, part, half=None):
            n = count if half is None else count // 2
            zs = pl.ds(first + (half or 0) * n, n)
            return buf.at[zs, row, part] if pair else buf.at[zs, part, row]

        def swap_rows():
            for direction, h in ways:
                at = piece(yp(-direction), mine)
                send(at, at, (zp(direction), y, x, c), swapped, swap_in)

        def swap_far():
            for direction, h in ways:
                at = piece(yp(2), mine, h)
                send(at, at, (zp(direction), y, x, c), swapped, swap_in)

        def done():
            wait(all3, swap_in)

        if m == "ou0":
            return swap_rows, swap_far, done
        sent = send_group(buf.at[some, 0] if pair else buf.at[some, :, 0])
        passed = send_group(whole)
        row_in, far_in = [new_sem(), new_sem()], [new_sem(), new_sem()]

        def a():
            for direction, h in ways:
                send(piece(y, mine), piece(y, mine), (z, yp(direction), x, c), sent, row_in[h])

        def b():
            for direction, h in ways:
                wait(whole, row_in[h])
                at = piece(yp(-direction), mine, h)
                send(at, at, (z, yp(direction), x, c), passed, far_in[h])
            swap_rows()

        def e():
            for _, h in ways:
                wait(part_half, far_in[h])
            swap_far()

        return a, b, e, done

    tp_sems = {}

    def gather_tp(buf, kind):
        if kind not in tp_sems:
            tp_sems[kind] = [(new_sem(), new_sem()) for _ in range(CHUNKS)]
        out = send_group(buf.at[pl.ds(0, TP - 1)])
        return [gather_chunk(buf, h, out, *tp_sems[kind][h]) for h in range(CHUNKS)]

    def gather_chunk(buf, h, out, chips, mate):
        me, other = buf.at[tp, h], (z, y, x, 1 - c)

        def slot(d):
            return buf.at[xp(d) * C + 1 - c, h]

        def begin():
            for d in (2, 1, -1):
                send(me, me, (z, y, xp(d), 1 - c), out, chips)
            send(me, me, other, out, mate)

        def forward():
            wait(buf.at[pl.ds(0, X - 1), h], chips)
            for d in (1, -1, 2):
                send(slot(d), slot(d), other, out, mate)

        def done():
            wait(buf.at[pl.ds(0, X), h], mate)

        return begin, forward, done

    rows_all, width = xs.shape
    cols = gx.shape[2] * 2
    nh = rows_all // CHUNKS
    last = CHUNKS - 1

    def normalise(layer, h):
        rows = pl.ds(h * nh, nh)

        def group(g):
            if layer == 0:
                return xs[rows, pl.ds(g * 128, 128)].astype(F32)
            return s1[g % TP, h, g // TP].astype(F32)

        total = None
        for g in range(width // 128):
            wide = group(g)
            total = wide * wide if total is None else total + wide * wide
        scale = lax.rsqrt(jnp.sum(total, axis=1, keepdims=True) / width + EPS)
        for g in range(width // 128):
            gain = ngain[pl.ds(layer, 1), pl.ds(g * 128, 128)]
            nb[rows, pl.ds(g * 128, 128)] = (group(g) * scale * gain).astype(BF16)

    def project(layer, buf, gb, h):
        n = nb[pl.ds(h * nh, nh), :]
        value = jnp.dot(n, buf[:, :, 0].reshape(width, cols), preferred_element_type=F32)
        gate = jnp.dot(n, buf[:, :, 1].reshape(width, cols), preferred_element_type=F32)
        gated = (value * sigmoid(gate)).astype(BF16)
        if h == last:
            gb[...] = gated[nh - HALO :]
        wide = gated.astype(F32)
        for j in range(2):
            gx[j, HALO + h * nh : HALO + h * nh + nh, :] = wide[:, j * 128 : (j + 1) * 128]

    def convolve(layer, f, h):
        first = h * nh + HALO - 30
        for j in range(2):
            acc = None
            for k in range(31):
                term = taps[k, pl.ds(layer, 1), pl.ds(j * 128, 128)] * gx[j, first + k : first + k + nh, :]
                acc = term if acc is None else acc + term
            f[tp, h, :, j * 128 : (j + 1) * 128] = acc.astype(BF16)

    def halo(gb, hbuf):
        copy = pltpu.make_async_remote_copy(
            src_ref=gb, dst_ref=hbuf, send_sem=new_sem(), recv_sem=new_sem(),
            device_id=after, device_id_type=MESH,
        )

        @pl.when(sp < Z * Y - 1)
        def _():
            copy.start()

        def arrives():
            @pl.when(sp > 0)
            def _():
                copy.wait_recv()
                for j in range(2):
                    gx[j, 0:HALO, :] = hbuf[:, j * 128 : (j + 1) * 128].astype(F32)

            @pl.when(sp == 0)
            def _():
                gx[:, 0:HALO, :] = jnp.zeros((2, HALO, 128), F32)

        def sent():
            @pl.when(sp < Z * Y - 1)
            def _():
                copy.wait_send()

        return arrives, sent

    def activate_and_project(layer, f, ou, nxt, h):
        first = second = jnp.zeros((nh, 128), F32)
        for k in range(TP):
            for j in range(2):
                part = f[k, h, :, j * 128 : (j + 1) * 128].astype(F32)
                first = first + part
                second = second + part * part
        mean = jnp.sum(first, axis=1, keepdims=True) / width
        var = jnp.sum(second, axis=1, keepdims=True) / width - mean * mean
        scale = lax.rsqrt(var + EPS)
        total = [jnp.zeros((nh, 128), F32) for _ in range(2)]
        for k in range(TP):
            v = (f[k, h].astype(F32) - mean) * scale * cg[k, pl.ds(layer, 1), :]
            act = (v * sigmoid(v)).astype(BF16)
            for hi in range(2):
                slot = lax.rem(tp + hi * TP + lax.rem(k - tp + 12, TP) + Z - 4, Z)
                w = ou[lax.div(slot, 2), lax.rem(slot, 2)].reshape(128, cols)
                total[hi] = total[hi] + lax.dot_general(
                    act, w, (((1,), (1,)), ((), ())), preferred_element_type=F32
                )
        for hi in range(2):
            if layer == 0:
                lane = pl.multiple_of((hi * TP + tp) * 128, 128)
                old = xs[pl.ds(h * nh, nh), pl.ds(lane, 128)]
            else:
                old = s1[tp, h, hi]
            nxt[tp, h, hi] = (old.astype(F32) + total[hi]).astype(BF16)

    perm_send = send_group(ow)
    perm_recv = new_sem()
    perm = [
        pltpu.make_async_remote_copy(
            src_ref=ow.at[layer], dst_ref=block(buf, to_z, y), send_sem=perm_send, recv_sem=perm_recv,
            device_id=goes_to, device_id_type=MESH,
        )
        for layer, buf in ((0, ou0), (1, ou1))
    ]
    drains.pop()
    stay = [pltpu.make_async_copy(ow.at[layer], block(buf, z, y), perm_recv) for layer, buf in ((0, ou0), (1, ou1))]

    def perm_start():
        @pl.when(far)
        def _():
            for copy in perm:
                copy.start()

        @pl.when(jnp.logical_not(far))
        def _():
            for copy in stay:
                copy.start()

    def perm_done():
        wait(ow, perm_recv)

    pass_vg, relay_vg, far_vg, near_vg, done_vg = y_group("vg0", vg0)
    pass_ou, relay_ou, far_ou, near_ou, done_ou = y_group("ou0", ou0)
    ou0_swap_rows, ou0_swap_far, ou0_done = spread("ou0", ou0)
    vg1_a, vg1_b, vg1_c, vg1_done = zip(*(spread("vg1", vg1, n, Z // 2) for n in (0, Z // 2)))
    ou1_a, ou1_b, ou1_c, ou1_done = spread("ou1", ou1)

    def vg0_stage(s):
        if s:
            z_wait("vg0", vg0, RING, s - 1)
        if s < 4:
            z_stage("vg0", vg0, RING, s)

    wait(vg0.at[z, y], own_sem[0])
    vg0_stage(0)
    pass_vg(0, [0])
    perm_start()
    wait(vg1.at[z, y], own_sem[1])
    z_stage("vg1", vg1, RING, 0)
    wait(cg.at[tp], own_sem[3])
    gain_sent, gain_in = send_group(cg.at[pl.ds(0, TP - 1)]), new_sem()
    for d in range(1, TP):
        to = lax.rem(tp + d, TP)
        send(cg.at[tp], cg.at[tp], (z, y, lax.div(to, C), lax.rem(to, C)), gain_sent, gain_in)
    wait(xs, own_sem[2])
    wait(ngain, own_sem[4])
    with scope("norm0"):
        for h in range(CHUNKS):
            normalise(0, h)

    ring = [[0]] + [brought(RING, s) for s in range(4)]

    def go_on(m, buf, plan, s):
        z_wait(m, buf, plan, s - 1)
        if s < len(plan):
            z_stage(m, buf, plan, s)

    def vg1_step(s):
        go_on("vg1", vg1, RING, s)

    def ou0_step(s):
        go_on("ou0", ou0, RING, s)

    def ou1_step(s):
        go_on("ou1", ou1, RING, s)

    even = [[d for d in ds if d % 2 == 0] for ds in ring]

    with scope("stage1"):
        vg0_stage(1)
        pass_vg(1, ring[1])
        relay_vg(0, ring[0])
        perm_done()
        z_stage("ou0", ou0, RING, 0)
        pass_ou(0, even[0])
    with scope("stage2"):
        vg0_stage(2)
        pass_vg(2, ring[2])
        relay_vg(1, ring[1])
        ou0_step(1)
        pass_ou(1, even[1])
        vg1_step(1)
    with scope("stage3"):
        vg0_stage(3)
        pass_vg(3, ring[3])
        relay_vg(2, ring[2])
        ou0_step(2)
        pass_ou(2, even[2])
        relay_ou(0, even[0])
        vg1_step(2)
    with scope("stage4"):
        vg0_stage(4)
        far_vg(4, ring[4])
        relay_vg(3, ring[3])
        ou0_step(3)
        pass_ou(3, even[3])
        relay_ou(1, even[1])
        vg1_step(3)
        z_stage("ou1", ou1, RING, 0)
    wait(taps, own_sem[5])
    with scope("vg0done"):
        near_vg(4, ring[4])
        done_vg()

    order = range(CHUNKS - 1, -1, -1)

    def receive(gather, h, between=None):
        if h == last:
            gather[h][1]()
            if between:
                between()
        if h:
            gather[h - 1][1]()
        gather[h][2]()

    def layer_of(layer, vg, gb, hbuf, f, ou, nxt, source, weights_ready, hooks):
        first, second = gather_tp(f, 1), gather_tp(nxt, 2)

        def hook(name):
            if name in hooks:
                with scope(name):
                    hooks[name]()

        for h in order:
            if source is not None:
                with scope("get%d" % h):
                    receive(source, h)
                normalise(layer, h)
            if h == last:
                weights_ready()
            with scope("proj%d" % h):
                project(layer, vg, gb, h)
            if h == last:
                arrives, sent = halo(gb, hbuf)
                hook("hookp")
            else:
                convolve(layer, f, h + 1)
                first[h + 1][0]()
                hook("head%d" % h)
        hook("hook0")
        with scope("halo"):
            arrives()
            convolve(layer, f, 0)
        first[0][0]()
        hook("hook0b")
        for h in order:
            with scope("ag%d" % h):
                receive(first, h, lambda: hook("hook1"))
            if h == last:
                hook("hook2")
            with scope("act%d" % h):
                activate_and_project(layer, f, ou, nxt, h)
            second[h][0]()
            hook("after%d" % h)
        return second, sent

    def hook0p():
        ou0_step(4)
        far_ou(4, even[4])
        relay_ou(2, even[2])
        relay_ou(3, even[3])
        ou1_step(1)

    def hook00():
        vg1_step(4)
        vg1_a[0]()

    def hook00b():
        near_ou(4, even[4])
        ou0_swap_rows()
        vg1_a[1]()
        ou1_step(2)

    def hook01():
        done_ou()
        ou0_swap_far()
        vg1_b[0]()
        ou1_step(3)

    def hook02():
        vg1_b[1]()
        wait(cg.at[pl.ds(0, TP - 1)], gain_in)
        ou0_done()

    def hook03():
        ou1_step(4)
        ou1_a()

    hooks0 = {
        "hookp": hook0p, "hook0": hook00, "hook0b": hook00b, "hook1": hook01, "hook2": hook02,
        "after3": vg1_c[0], "after2": vg1_c[1], "after1": hook03,
    }
    rest, sent0 = layer_of(0, vg0, gb0, h0, f0, ou0, s1, None, lambda: None, hooks0)

    def ready():
        with scope("vg1done"):
            ou1_b()
            vg1_done[0]()
            vg1_done[1]()

    hooks1 = {"head1": ou1_c, "hook2": ou1_done}
    rest1, sent1 = layer_of(1, vg1, gb1, h1, f1, ou1, s2, rest, ready, hooks1)
    for h in order:
        with scope("last%d" % h):
            receive(rest1, h)
        for g in range(width // 128):
            out_ref[h * nh : (h + 1) * nh, g * 128 : (g + 1) * 128] = s2[g % TP, h, g // TP]

    with scope("out"):
        for ref, sem in drains:
            wait(ref, sem)
        sent0()
        sent1()

        @pl.when(far)
        def _():
            wait(ow, perm_send)

    assert used[0] == N_SEMS, used[0]


def body(stream_in, norm_gain, value_weight, gate_weight, conv_taps, channel_gain, out_weight):
    rows, width = stream_in.shape
    depth, cols = value_weight.shape[1:]
    hbm, vmem = pl.BlockSpec(memory_space=pltpu.HBM), pl.BlockSpec(memory_space=pltpu.VMEM)
    out_t = jnp.swapaxes(out_weight, 1, 2)
    taps = jnp.swapaxes(conv_taps, 0, 1)
    return pl.pallas_call(
        kernel,
        out_shape=pltpu.VMEM((rows, width), BF16),
        in_specs=[hbm] * 7,
        out_specs=vmem,
        scratch_shapes=[
            pltpu.VMEM(taps.shape, F32),
            pltpu.VMEM(norm_gain.shape, F32),
            pltpu.VMEM((Z, Y, 2, depth, cols), BF16),
            pltpu.VMEM((Z, Y, 2, depth, cols), BF16),
            pltpu.VMEM((Z // 2, 2, Y, depth, cols), BF16),
            pltpu.VMEM((Z // 2, 2, Y, depth, cols), BF16),
            pltpu.VMEM((rows, width), BF16),
            pltpu.VMEM((TP, CHUNKS, 2, rows // CHUNKS, 128), BF16),
            pltpu.VMEM((TP, CHUNKS, 2, rows // CHUNKS, 128), BF16),
            pltpu.VMEM((TP, CHUNKS, rows // CHUNKS, cols), BF16),
            pltpu.VMEM((TP, CHUNKS, rows // CHUNKS, cols), BF16),
            pltpu.VMEM((rows, width), BF16),
            pltpu.VMEM((2, rows + HALO, 128), F32),
            pltpu.VMEM((HALO, cols), BF16),
            pltpu.VMEM((HALO, cols), BF16),
            pltpu.VMEM((HALO, cols), BF16),
            pltpu.VMEM((HALO, cols), BF16),
            pltpu.VMEM((TP, 2, cols), F32),
            pltpu.SemaphoreType.DMA((N_SEMS,)),
        ],
        compiler_params=pltpu.CompilerParams(
            collective_id=0, has_side_effects=True, vmem_limit_bytes=VMEM_LIMIT
        ),
    )(stream_in, norm_gain, value_weight, gate_weight, taps, channel_gain, out_t)


def solution(mesh):
    finer = Mesh(mesh.devices.reshape(Z, Y, X, C), ("z", "y", "x", "c"))
    sp, tp = ("z", "y"), ("x", "c")
    placed = (
        P(sp, None),
        P(),
        P(None, sp, tp),
        P(None, sp, tp),
        P(None, None, tp),
        P(None, tp),
        P(None, tp, sp),
    )
    return jax.shard_map(body, mesh=finer, in_specs=placed, out_specs=P(sp, None), check_vma=False)
```

```python
import jax
import jax.numpy as jnp
from jax import lax
from jax.experimental import pallas as pl
from jax.experimental.pallas import tpu as pltpu
from jax.sharding import Mesh
from jax.sharding import PartitionSpec as P

Z, Y, X, C = 16, 4, 4, 2
TP = X * C
MESH = pl.DeviceIdType.MESH
EPS = 1e-05
F32 = jnp.float32
BF16 = jnp.bfloat16
N_SEMS = 106
HALO = 32
RING = [
    [(2 * s, tuple(d for d in (2 * s + 2, 2 * s + 1) if d <= Z // 2)),
     (-2 * s, tuple(-d for d in (2 * s + 2, 2 * s + 1) if d < Z // 2))]
    for s in range(4)
]
VMEM_LIMIT = 60_000_000
CHUNKS = 4
scope = jax.named_scope


def sigmoid(v):
    return 0.5 + 0.5 * jnp.tanh(0.5 * v)


def kernel(
    stream_hbm, ngain_hbm, vw, gw, taps_hbm, cgain, ow, out_ref,
    taps, ngain, vg0, vg1, ou0, ou1, xs, s1, s2, f0, f1, nb, gx, h0, h1, gb0, gb1, cg, sems,
):
    z, y, x, c = (lax.axis_index(a) for a in ("z", "y", "x", "c"))
    tp = x * C + c
    sp = z * Y + y
    used = [0]

    def new_sem():
        used[0] += 1
        return sems.at[used[0] - 1]

    def send(src, dst, device, send_sem, recv_sem):
        pltpu.make_async_remote_copy(
            src_ref=src, dst_ref=dst, send_sem=send_sem, recv_sem=recv_sem,
            device_id=device, device_id_type=MESH,
        ).start()

    def wait(ref, sem):
        pltpu.make_async_copy(ref, ref, sem).wait()

    drains = []

    def send_group(ref):
        sem = new_sem()
        drains.append((ref, sem))
        return sem

    def zp(d):
        return lax.rem(z + d + Z, Z)

    def yp(d):
        return lax.rem(y + d + Y, Y)

    def xp(d):
        return lax.rem(x + d + X, X)

    own_sem = [new_sem() for _ in range(6)]
    own = [
        pltpu.make_async_copy(vw.at[0], vg0.at[z, y, 0], own_sem[0]),
        pltpu.make_async_copy(gw.at[0], vg0.at[z, y, 1], own_sem[0]),
        pltpu.make_async_copy(vw.at[1], vg1.at[z, y, 0], own_sem[1]),
        pltpu.make_async_copy(gw.at[1], vg1.at[z, y, 1], own_sem[1]),
        pltpu.make_async_copy(stream_hbm, xs, own_sem[2]),
        pltpu.make_async_copy(cgain, cg.at[tp], own_sem[3]),
        pltpu.make_async_copy(ngain_hbm, ngain, own_sem[4]),
        pltpu.make_async_copy(taps_hbm, taps, own_sem[5]),
    ]
    for copy in own:
        copy.start()

    zlo = lax.rem(z, TP)
    far = zlo != tp
    to_z = zp(lax.rem(tp - zlo + 12, TP) - 4)
    from_z = zp(4 - lax.rem(zlo - tp + 12, TP))
    goes_to = (to_z, y, lax.div(zlo, C), lax.rem(zlo, C))
    comes_from = (from_z, y, lax.div(zlo, C), lax.rem(zlo, C))
    nsp = lax.rem(sp + 1, Z * Y)
    psp = lax.rem(sp + Z * Y - 1, Z * Y)
    after = (lax.div(nsp, Y), lax.rem(nsp, Y), x, c)
    before = (lax.div(psp, Y), lax.rem(psp, Y), x, c)

    barrier = pltpu.get_barrier_semaphore()
    peers = [(zp(d), y, x, c) for d in (1, 2, -1, -2)] + [(z, yp(d), x, c) for d in (1, -1, 2)]
    for d in range(1, TP):
        other = lax.rem(tp + d, TP)
        peers.append((z, y, lax.div(other, C), lax.rem(other, C)))
    peers += [after, before]
    for peer in peers:
        pl.semaphore_signal(barrier, inc=1, device_id=peer, device_id_type=MESH)

    @pl.when(far)
    def _():
        pl.semaphore_signal(barrier, inc=1, device_id=comes_from, device_id_type=MESH)

    with scope("barrier"):
        pl.semaphore_wait(barrier, len(peers) + jnp.where(far, 1, 0))

    def block(buf, slot, row, part=None):
        if buf.shape[0] != Z:
            return buf.at[lax.div(slot, 2), lax.rem(slot, 2), row]
        return buf.at[slot, row] if part is None else buf.at[slot, row, part]

    def blocks(buf, n, part=None):
        if buf.shape[0] != Z:
            return buf.at[pl.ds(0, max(1, n // 3)), 0, pl.ds(0, 3)] if n % 3 == 0 else buf.at[pl.ds(0, 1), 0, pl.ds(0, n)]
        return buf.at[pl.ds(0, n), 0] if part is None else buf.at[pl.ds(0, n), 0, part]

    z_sems = {}

    def brought(plan, s):
        return [d for _, news in plan[s] for d in news]

    def z_stage(m, buf, plan, s, part=None):
        if s == 0:
            z_sems[m, part] = [new_sem() for _ in plan], send_group(blocks(buf, Z - 1, part))
        sems_in, out = z_sems[m, part]
        for d, news in plan[s]:
            at = block(buf, zp(-d), y, part)
            for new in news:
                send(at, at, (zp(new - d), y, x, c), out, sems_in[s])

    def z_wait(m, buf, plan, s, part=None):
        wait(blocks(buf, len(brought(plan, s)), part), z_sems[m, part][0][s])

    def y_group(m, buf):
        pair = buf.shape[0] == Z
        sent = send_group(buf.at[:, pl.ds(0, 2)] if pair else buf.at[pl.ds(0, 4), 0])
        far_bytes = buf.at[:, 0] if pair else buf.at[pl.ds(0, 2), 0]
        passed, far_in, near_in = send_group(far_bytes), new_sem(), {}

        def half(slot, row, h):
            return buf.at[slot, row, h] if pair else block(buf, slot, row).at[pl.ds(h * 16, 16)]

        def pass_on(key, ds):
            near_in[key] = new_sem(), new_sem()
            for d in ds:
                at = block(buf, zp(-d), y)
                for direction, sem in zip((1, -1), near_in[key]):
                    send(at, at, (z, yp(direction), x, c), sent, sem)

        def relay(key, ds):
            for direction, h in ((1, 0), (-1, 1)):
                wait(blocks(buf, len(ds)), near_in[key][h])
                for d in ds:
                    at = half(zp(-d), yp(-direction), h)
                    send(at, at, (z, yp(direction), x, c), passed, far_in)

        def pass_far(key, ds):
            pass_on(key, ds)
            for d in ds:
                at = block(buf, zp(-d), y)
                send(at, at, (z, yp(2), x, c), passed, far_in)

        def near_done(key, ds):
            for sem in near_in[key]:
                wait(blocks(buf, len(ds)), sem)

        def done():
            wait(far_bytes, far_in)

        return pass_on, relay, pass_far, near_done, done

    mine = lax.rem(z, 2)

    def spread(m, buf, first=0, count=None):
        pair = buf.shape[0] == Z
        count = count or buf.shape[0]
        some = pl.ds(first, count)
        whole = buf.at[some, 0, 0]
        part_half = buf.at[pl.ds(first, count // 2), 0, 0]
        all3 = buf.at[some, pl.ds(0, 3), 0] if pair else buf.at[some, 0, pl.ds(0, 3)]
        swapped, swap_in = send_group(all3), new_sem()
        ways = ((1, 0), (-1, 1))

        def piece(row, part, half=None):
            n = count if half is None else count // 2
            zs = pl.ds(first + (half or 0) * n, n)
            return buf.at[zs, row, part] if pair else buf.at[zs, part, row]

        def swap_rows():
            for direction, h in ways:
                at = piece(yp(-direction), mine)
                send(at, at, (zp(direction), y, x, c), swapped, swap_in)

        def swap_far():
            for direction, h in ways:
                at = piece(yp(2), mine, h)
                send(at, at, (zp(direction), y, x, c), swapped, swap_in)

        def done():
            wait(all3, swap_in)

        if m == "ou0":
            return swap_rows, swap_far, done
        sent = send_group(buf.at[some, 0] if pair else buf.at[some, :, 0])
        passed = send_group(whole)
        row_in, far_in = [new_sem(), new_sem()], [new_sem(), new_sem()]

        def a():
            for direction, h in ways:
                send(piece(y, mine), piece(y, mine), (z, yp(direction), x, c), sent, row_in[h])

        def b():
            for direction, h in ways:
                wait(whole, row_in[h])
                at = piece(yp(-direction), mine, h)
                send(at, at, (z, yp(direction), x, c), passed, far_in[h])
            swap_rows()

        def e():
            for _, h in ways:
                wait(part_half, far_in[h])
            swap_far()

        return a, b, e, done

    tp_sems = {}

    def gather_tp(buf, kind):
        if kind not in tp_sems:
            tp_sems[kind] = [(new_sem(), new_sem()) for _ in range(CHUNKS)]
        out = send_group(buf.at[pl.ds(0, TP - 1)])
        return [gather_chunk(buf, h, out, *tp_sems[kind][h]) for h in range(CHUNKS)]

    def gather_chunk(buf, h, out, chips, mate):
        me, other = buf.at[tp, h], (z, y, x, 1 - c)

        def slot(d):
            return buf.at[xp(d) * C + 1 - c, h]

        def begin():
            for d in (2, 1, -1):
                send(me, me, (z, y, xp(d), 1 - c), out, chips)
            send(me, me, other, out, mate)

        def forward():
            wait(buf.at[pl.ds(0, X - 1), h], chips)
            for d in (1, -1, 2):
                send(slot(d), slot(d), other, out, mate)

        def done():
            wait(buf.at[pl.ds(0, X), h], mate)

        return begin, forward, done

    rows_all, width = xs.shape
    cols = gx.shape[2] * 2
    nh = rows_all // CHUNKS
    last = CHUNKS - 1

    def normalise(layer, h):
        rows = pl.ds(h * nh, nh)

        def group(g):
            if layer == 0:
                return xs[rows, pl.ds(g * 128, 128)].astype(F32)
            return s1[g % TP, h, g // TP].astype(F32)

        total = None
        for g in range(width // 128):
            wide = group(g)
            total = wide * wide if total is None else total + wide * wide
        scale = lax.rsqrt(jnp.sum(total, axis=1, keepdims=True) / width + EPS)
        for g in range(width // 128):
            gain = ngain[pl.ds(layer, 1), pl.ds(g * 128, 128)]
            nb[rows, pl.ds(g * 128, 128)] = (group(g) * scale * gain).astype(BF16)

    def project(layer, buf, gb, h):
        n = nb[pl.ds(h * nh, nh), :]
        value = jnp.dot(n, buf[:, :, 0].reshape(width, cols), preferred_element_type=F32)
        gate = jnp.dot(n, buf[:, :, 1].reshape(width, cols), preferred_element_type=F32)
        gated = (value * sigmoid(gate)).astype(BF16)
        if h == last:
            gb[...] = gated[nh - HALO :]
        wide = gated.astype(F32)
        for j in range(2):
            gx[j, HALO + h * nh : HALO + h * nh + nh, :] = wide[:, j * 128 : (j + 1) * 128]

    def convolve(layer, f, h):
        first = h * nh + HALO - 30
        for j in range(2):
            acc = None
            for k in range(31):
                term = taps[k, pl.ds(layer, 1), pl.ds(j * 128, 128)] * gx[j, first + k : first + k + nh, :]
                acc = term if acc is None else acc + term
            f[tp, h, :, j * 128 : (j + 1) * 128] = acc.astype(BF16)

    def halo(gb, hbuf):
        copy = pltpu.make_async_remote_copy(
            src_ref=gb, dst_ref=hbuf, send_sem=new_sem(), recv_sem=new_sem(),
            device_id=after, device_id_type=MESH,
        )

        @pl.when(sp < Z * Y - 1)
        def _():
            copy.start()

        def arrives():
            @pl.when(sp > 0)
            def _():
                copy.wait_recv()
                for j in range(2):
                    gx[j, 0:HALO, :] = hbuf[:, j * 128 : (j + 1) * 128].astype(F32)

            @pl.when(sp == 0)
            def _():
                gx[:, 0:HALO, :] = jnp.zeros((2, HALO, 128), F32)

        def sent():
            @pl.when(sp < Z * Y - 1)
            def _():
                copy.wait_send()

        return arrives, sent

    def activate_and_project(layer, f, ou, nxt, h):
        first = second = jnp.zeros((nh, 128), F32)
        for k in range(TP):
            for j in range(2):
                part = f[k, h, :, j * 128 : (j + 1) * 128].astype(F32)
                first = first + part
                second = second + part * part
        mean = jnp.sum(first, axis=1, keepdims=True) / width
        var = jnp.sum(second, axis=1, keepdims=True) / width - mean * mean
        scale = lax.rsqrt(var + EPS)
        total = [jnp.zeros((nh, 128), F32) for _ in range(2)]
        for k in range(TP):
            v = (f[k, h].astype(F32) - mean) * scale * cg[k, pl.ds(layer, 1), :]
            act = (v * sigmoid(v)).astype(BF16)
            for hi in range(2):
                slot = lax.rem(tp + hi * TP + lax.rem(k - tp + 12, TP) + Z - 4, Z)
                w = ou[lax.div(slot, 2), lax.rem(slot, 2)].reshape(128, cols)
                total[hi] = total[hi] + lax.dot_general(
                    act, w, (((1,), (1,)), ((), ())), preferred_element_type=F32
                )
        for hi in range(2):
            if layer == 0:
                lane = pl.multiple_of((hi * TP + tp) * 128, 128)
                old = xs[pl.ds(h * nh, nh), pl.ds(lane, 128)]
            else:
                old = s1[tp, h, hi]
            nxt[tp, h, hi] = (old.astype(F32) + total[hi]).astype(BF16)

    perm_send = send_group(ow)
    perm_recv = new_sem()
    perm = [
        pltpu.make_async_remote_copy(
            src_ref=ow.at[layer], dst_ref=block(buf, to_z, y), send_sem=perm_send, recv_sem=perm_recv,
            device_id=goes_to, device_id_type=MESH,
        )
        for layer, buf in ((0, ou0), (1, ou1))
    ]
    drains.pop()
    stay = [pltpu.make_async_copy(ow.at[layer], block(buf, z, y), perm_recv) for layer, buf in ((0, ou0), (1, ou1))]

    def perm_start():
        @pl.when(far)
        def _():
            for copy in perm:
                copy.start()

        @pl.when(jnp.logical_not(far))
        def _():
            for copy in stay:
                copy.start()

    def perm_done():
        wait(ow, perm_recv)

    pass_vg, relay_vg, far_vg, near_vg, done_vg = y_group("vg0", vg0)
    pass_ou, relay_ou, far_ou, near_ou, done_ou = y_group("ou0", ou0)
    ou0_swap_rows, ou0_swap_far, ou0_done = spread("ou0", ou0)
    vg1_a, vg1_b, vg1_c, vg1_done = zip(*(spread("vg1", vg1, n, Z // 2) for n in (0, Z // 2)))
    ou1_a, ou1_b, ou1_c, ou1_done = spread("ou1", ou1)

    def vg0_stage(s):
        if s:
            z_wait("vg0", vg0, RING, s - 1)
        if s < 4:
            z_stage("vg0", vg0, RING, s)

    wait(vg0.at[z, y], own_sem[0])
    vg0_stage(0)
    pass_vg(0, [0])
    perm_start()
    wait(vg1.at[z, y], own_sem[1])
    z_stage("vg1", vg1, RING, 0)
    wait(cg.at[tp], own_sem[3])
    gain_sent, gain_in = send_group(cg.at[pl.ds(0, TP - 1)]), new_sem()
    for d in range(1, TP):
        to = lax.rem(tp + d, TP)
        send(cg.at[tp], cg.at[tp], (z, y, lax.div(to, C), lax.rem(to, C)), gain_sent, gain_in)
    wait(xs, own_sem[2])
    wait(ngain, own_sem[4])
    with scope("norm0"):
        for h in range(CHUNKS):
            normalise(0, h)

    ring = [[0]] + [brought(RING, s) for s in range(4)]

    def go_on(m, buf, plan, s):
        z_wait(m, buf, plan, s - 1)
        if s < len(plan):
            z_stage(m, buf, plan, s)

    def vg1_step(s):
        go_on("vg1", vg1, RING, s)

    def ou0_step(s):
        go_on("ou0", ou0, RING, s)

    def ou1_step(s):
        go_on("ou1", ou1, RING, s)

    even = [[d for d in ds if d % 2 == 0] for ds in ring]

    with scope("stage1"):
        vg0_stage(1)
        pass_vg(1, ring[1])
        relay_vg(0, ring[0])
        perm_done()
        z_stage("ou0", ou0, RING, 0)
        pass_ou(0, even[0])
    with scope("stage2"):
        vg0_stage(2)
        pass_vg(2, ring[2])
        relay_vg(1, ring[1])
        ou0_step(1)
        pass_ou(1, even[1])
        vg1_step(1)
    with scope("stage3"):
        vg0_stage(3)
        pass_vg(3, ring[3])
        relay_vg(2, ring[2])
        ou0_step(2)
        pass_ou(2, even[2])
        relay_ou(0, even[0])
        vg1_step(2)
        z_stage("ou1", ou1, RING, 0)
    with scope("stage4"):
        vg0_stage(4)
        far_vg(4, ring[4])
        relay_vg(3, ring[3])
        ou0_step(3)
        pass_ou(3, even[3])
        relay_ou(1, even[1])
        vg1_step(3)
        ou1_step(1)
    wait(taps, own_sem[5])
    with scope("vg0done"):
        near_vg(4, ring[4])
        done_vg()

    order = range(CHUNKS - 1, -1, -1)

    def receive(gather, h, between=None):
        if h == last:
            gather[h][1]()
            if between:
                between()
        if h:
            gather[h - 1][1]()
        gather[h][2]()

    def layer_of(layer, vg, gb, hbuf, f, ou, nxt, source, weights_ready, hooks):
        first, second = gather_tp(f, 1), gather_tp(nxt, 2)

        def hook(name):
            if name in hooks:
                with scope(name):
                    hooks[name]()

        for h in order:
            if source is not None:
                with scope("get%d" % h):
                    receive(source, h)
                normalise(layer, h)
            if h == last:
                weights_ready()
            with scope("proj%d" % h):
                project(layer, vg, gb, h)
            if h == last:
                arrives, sent = halo(gb, hbuf)
                hook("hookp")
            else:
                convolve(layer, f, h + 1)
                first[h + 1][0]()
                hook("head%d" % h)
        hook("hook0")
        with scope("halo"):
            arrives()
            convolve(layer, f, 0)
        first[0][0]()
        hook("hook0b")
        for h in order:
            with scope("ag%d" % h):
                receive(first, h, lambda: hook("hook1"))
            if h == last:
                hook("hook2")
            with scope("act%d" % h):
                activate_and_project(layer, f, ou, nxt, h)
            second[h][0]()
            hook("after%d" % h)
        return second, sent

    def hook0p():
        ou0_step(4)
        far_ou(4, even[4])
        relay_ou(2, even[2])
        relay_ou(3, even[3])
        ou1_step(2)

    def head02():
        vg1_step(4)
        vg1_a[0]()

    def hook00():
        vg1_a[1]()

    def hook00b():
        near_ou(4, even[4])
        ou0_swap_rows()
        ou1_step(3)
        done_ou()
        ou0_swap_far()

    def hook01():
        vg1_b[0]()

    def hook02():
        vg1_b[1]()
        wait(cg.at[pl.ds(0, TP - 1)], gain_in)
        ou0_done()

    def hook03():
        ou1_step(4)
        ou1_a()

    hooks0 = {
        "hookp": hook0p, "head2": head02, "hook0": hook00, "hook0b": hook00b, "hook1": hook01, "hook2": hook02,
        "after3": vg1_c[0], "after2": vg1_c[1], "after1": hook03,
    }
    rest, sent0 = layer_of(0, vg0, gb0, h0, f0, ou0, s1, None, lambda: None, hooks0)

    def ready():
        with scope("vg1done"):
            ou1_b()
            vg1_done[0]()
            vg1_done[1]()

    hooks1 = {"head1": ou1_c, "hook2": ou1_done}
    rest1, sent1 = layer_of(1, vg1, gb1, h1, f1, ou1, s2, rest, ready, hooks1)
    for h in order:
        with scope("last%d" % h):
            receive(rest1, h)
        for g in range(width // 128):
            out_ref[h * nh : (h + 1) * nh, g * 128 : (g + 1) * 128] = s2[g % TP, h, g // TP]

    with scope("out"):
        for ref, sem in drains:
            wait(ref, sem)
        sent0()
        sent1()

        @pl.when(far)
        def _():
            wait(ow, perm_send)

    assert used[0] == N_SEMS, used[0]


def body(stream_in, norm_gain, value_weight, gate_weight, conv_taps, channel_gain, out_weight):
    rows, width = stream_in.shape
    depth, cols = value_weight.shape[1:]
    hbm, vmem = pl.BlockSpec(memory_space=pltpu.HBM), pl.BlockSpec(memory_space=pltpu.VMEM)
    out_t = jnp.swapaxes(out_weight, 1, 2)
    taps = jnp.swapaxes(conv_taps, 0, 1)
    return pl.pallas_call(
        kernel,
        out_shape=pltpu.VMEM((rows, width), BF16),
        in_specs=[hbm] * 7,
        out_specs=vmem,
        scratch_shapes=[
            pltpu.VMEM(taps.shape, F32),
            pltpu.VMEM(norm_gain.shape, F32),
            pltpu.VMEM((Z, Y, 2, depth, cols), BF16),
            pltpu.VMEM((Z, Y, 2, depth, cols), BF16),
            pltpu.VMEM((Z // 2, 2, Y, depth, cols), BF16),
            pltpu.VMEM((Z // 2, 2, Y, depth, cols), BF16),
            pltpu.VMEM((rows, width), BF16),
            pltpu.VMEM((TP, CHUNKS, 2, rows // CHUNKS, 128), BF16),
            pltpu.VMEM((TP, CHUNKS, 2, rows // CHUNKS, 128), BF16),
            pltpu.VMEM((TP, CHUNKS, rows // CHUNKS, cols), BF16),
            pltpu.VMEM((TP, CHUNKS, rows // CHUNKS, cols), BF16),
            pltpu.VMEM((rows, width), BF16),
            pltpu.VMEM((2, rows + HALO, 128), F32),
            pltpu.VMEM((HALO, cols), BF16),
            pltpu.VMEM((HALO, cols), BF16),
            pltpu.VMEM((HALO, cols), BF16),
            pltpu.VMEM((HALO, cols), BF16),
            pltpu.VMEM((TP, 2, cols), F32),
            pltpu.SemaphoreType.DMA((N_SEMS,)),
        ],
        compiler_params=pltpu.CompilerParams(
            collective_id=0, has_side_effects=True, vmem_limit_bytes=VMEM_LIMIT
        ),
    )(stream_in, norm_gain, value_weight, gate_weight, taps, channel_gain, out_t)


def solution(mesh):
    finer = Mesh(mesh.devices.reshape(Z, Y, X, C), ("z", "y", "x", "c"))
    sp, tp = ("z", "y"), ("x", "c")
    placed = (
        P(sp, None),
        P(),
        P(None, sp, tp),
        P(None, sp, tp),
        P(None, None, tp),
        P(None, tp),
        P(None, tp, sp),
    )
    return jax.shard_map(body, mesh=finer, in_specs=placed, out_specs=P(sp, None), check_vma=False)
```
